32 devices in a mesh: tp: 8 (over z, y), dp: 4 (over x, core).
Axes of the slice: x: 2, y: 2, z: 4, core: 2. Of those that a mesh axis runs over, the one named last changes fastest.
Arguments:
- tokens: bfloat16 [96, 1024], P('tp', 'dp'), may hold values from -6 to 6
- lengths: int32 [96], P('dp'), may hold values from 1 to 8, 192 in all
- norm_gain: float32 [2, 1024], P(None, 'dp'), may hold values from 0.1 to 1.9
- w_gate: bfloat16 [2, 1024, 512], P(None, 'dp', 'tp'), may hold values from -0.1875 to 0.1875
- w_value: bfloat16 [2, 1024, 512], P(None, 'dp', 'tp'), may hold values from -0.1875 to 0.1875
- w_write: bfloat16 [2, 1024, 256], P(None, 'dp', 'tp'), may hold values from -0.1875 to 0.1875
- w_read: bfloat16 [2, 1024, 256], P(None, 'dp', 'tp'), may hold values from -0.1875 to 0.1875
- w_step: bfloat16 [2, 1024, 8], P(None, 'dp', 'tp'), may hold values from -0.1875 to 0.1875
- step_bias: float32 [2, 8], P(None, 'tp'), may hold values from -1 to 1
- decay_rate: float32 [2, 8], P(None, 'tp'), may hold values from 0.5 to 4
- skip_gain: float32 [2, 8], P(None, 'tp'), may hold values from 0.5 to 2
- conv_value_w: float32 [2, 4, 512], P(None, None, 'tp'), may hold values from -3 to 3
- conv_write_w: float32 [2, 4, 256], P(None, None, 'tp'), may hold values from -3 to 3
- conv_read_w: float32 [2, 4, 256], P(None, None, 'tp'), may hold values from -3 to 3
- group_gain: float32 [2, 512], P(None, 'tp'), may hold values from 0.1 to 1.9
- w_out: bfloat16 [2, 512, 1024], P(None, 'tp', 'dp'), may hold values from -0.25 to 0.25
- state: float32 [2, 96, 8, 64, 128], P(None, 'dp', 'tp'), may hold values from -0.6 to 0.6
- hist_value: bfloat16 [2, 96, 3, 512], P(None, 'dp', None, 'tp'), may hold values from -6 to 6
- hist_write: bfloat16 [2, 96, 3, 256], P(None, 'dp', None, 'tp'), may hold values from -6 to 6
- hist_read: bfloat16 [2, 96, 3, 256], P(None, 'dp', None, 'tp'), may hold values from -6 to 6
Outputs:
- mixed: float32 [96, 1024], P('tp', 'dp')
- new_state: float32 [2, 96, 8, 64, 128], P(None, 'dp', 'tp')
- new_hist_value: bfloat16 [2, 96, 3, 512], P(None, 'dp', None, 'tp')
- new_hist_write: bfloat16 [2, 96, 3, 256], P(None, 'dp', None, 'tp')
- new_hist_read: bfloat16 [2, 96, 3, 256], P(None, 'dp', None, 'tp')
The draws below stay inside these ranges and needn't reach their ends.
Inputs may be any that keep to these rules, and one draw needn't show every extreme that they name: `lengths`: each sequence holds between 1 and 8 tokens before this step, and some sequence holds exactly 8.
All inputs are finite; a program needn't handle non-finite values.
Results may differ from the reference program's by a relative error of at most 0.03.
Values may be sent and summed in bfloat16 or wider, within the bound.
A program may use at most 64 MiB of HBM per device.

```python
import math
import jax
import jax.numpy as jnp
import numpy as np
from jax import lax

D = 1024
HEAD_DIM = 64
STATE = 128
GROUPS = 2
KERNEL = 4
HEADS = 8
WIDTH = 512
SEQS = 96


def block_levels(own_key, dims, split, low, high):
    def one(position, blocks):
        draws = jax.random.uniform(jax.random.fold_in(jax.random.fold_in(own_key, 6), position), (blocks,), jnp.float32, low / len(split), high / len(split))
        return jnp.repeat(jnp.exp(draws), dims[position] // blocks).reshape((-1,) + (1,) * (len(dims) - position - 1))

    loudness = one(*split[0])
    for cut in split[1:]:
        loudness = loudness * one(*cut)
    return loudness


def profile(count, total, reach, lean):
    loads = [(1 << 20) // math.isqrt(rank ** lean) + 1 for rank in range(2, count + 1)]
    rest, given = total - reach - (count - 1), [1] * (count - 1)
    while rest > 0:
        free = [i for i in range(count - 1) if given[i] < reach]
        whole, left = sum([loads[i] for i in free]), rest
        for i in free:
            more = min(reach - given[i], max(1, left * loads[i] // whole), rest)
            given[i] = given[i] + more
            rest = rest - more
    return np.array([reach] + given)


def ragged(rng, number_of, total, limit, skew):
    if number_of == 2:
        one = jax.random.randint(rng, (), max(1, total - limit), min(limit, total - 1) + 1)
        return jnp.stack([one, total - one])
    tallies = jnp.asarray(profile(number_of, total, limit, skew), jnp.int32)
    pairs = (number_of - 1) // 2
    source_of, receiver = tallies[1:1 + 2 * pairs:2], tallies[2:2 + 2 * pairs:2]
    room = jnp.minimum(source_of - 1, limit - receiver)
    moved = jax.random.randint(jax.random.fold_in(rng, 1), (pairs,), 0, 1 << 20) % (room + 1)
    tallies = tallies.at[1:1 + 2 * pairs:2].set(source_of - moved).at[2:2 + 2 * pairs:2].set(receiver + moved)
    return tallies[jax.random.permutation(jax.random.fold_in(rng, 2), number_of)]


def noise(stream_key, dims, width, bound, cuts=(), kind=jnp.bfloat16):
    level = block_levels(stream_key, dims, cuts, -0.22, 0.18) if cuts else 1.0
    values = jax.random.normal(stream_key, dims, jnp.float32) * width * level
    return jnp.minimum(jnp.maximum(values, -bound), bound).astype(kind)


def setup_inputs(seed: int = 0) -> dict:
    key_list = jax.random.split(jax.random.key(seed), 21)
    tokens = noise(key_list[0], (SEQS, D), 1.0, 6.0, ((0, 8), (1, 4)))
    lengths = ragged(key_list[1], SEQS, 2 * SEQS, 8, 2).astype(jnp.int32)
    norm_gain = jnp.clip(1.0 + 0.18 * jax.random.normal(key_list[2], (2, D), jnp.float32), 0.1, 1.9)
    w_gate = noise(key_list[3], (2, D, WIDTH), D ** -0.5, 0.1875, ((1, 4), (2, 8)))
    w_value = noise(key_list[4], (2, D, WIDTH), D ** -0.5, 0.1875, ((1, 4), (2, 8)))
    w_write = noise(key_list[5], (2, D, GROUPS * STATE), D ** -0.5, 0.1875, ((1, 4), (2, 8)))
    w_read = noise(key_list[6], (2, D, GROUPS * STATE), D ** -0.5, 0.1875, ((1, 4), (2, 8)))
    w_step = noise(key_list[7], (2, D, HEADS), D ** -0.5, 0.1875, ((1, 4), (2, 8)))
    step_bias = jnp.clip(jax.random.uniform(key_list[8], (2, HEADS), jnp.float32, -1.0, 1.0) * block_levels(key_list[8], (2, HEADS), ((1, 8),), -0.4, 0.0), -1.0, 1.0)
    decay_rate = jnp.clip(jnp.exp(math.log(4.0) - 2.0794415 * jax.random.uniform(key_list[9], (2, HEADS), jnp.float32) ** block_levels(key_list[9], (2, HEADS), ((1, 8),), -0.2, 0.2)), 0.5, 4.0)
    skip_gain = jnp.clip(0.5 + 1.5 * jax.random.uniform(key_list[10], (2, HEADS), jnp.float32) ** block_levels(key_list[10], (2, HEADS), ((1, 8),), -0.2, 0.2), 0.5, 2.0)
    conv_value_w = noise(key_list[11], (2, KERNEL, WIDTH), KERNEL ** -0.5, 3.0, ((2, 8),), jnp.float32)
    conv_write_w = noise(key_list[12], (2, KERNEL, GROUPS * STATE), KERNEL ** -0.5, 3.0, ((2, 8),), jnp.float32)
    conv_read_w = noise(key_list[13], (2, KERNEL, GROUPS * STATE), KERNEL ** -0.5, 3.0, ((2, 8),), jnp.float32)
    group_gain = jnp.clip(1.0 + 0.18 * jax.random.normal(key_list[14], (2, WIDTH), jnp.float32), 0.1, 1.9)
    w_out = noise(key_list[15], (2, WIDTH, D), WIDTH ** -0.5, 0.25, ((1, 8), (2, 4)))
    state = noise(key_list[16], (2, SEQS, HEADS, HEAD_DIM, STATE), 0.1, 0.6, ((1, 4), (2, 8)), jnp.float32)
    hist_value = noise(key_list[17], (2, SEQS, KERNEL - 1, WIDTH), 1.0, 6.0, ((1, 4), (3, 8)))
    hist_write = noise(key_list[18], (2, SEQS, KERNEL - 1, GROUPS * STATE), 1.0, 6.0, ((1, 4), (3, 8)))
    hist_read = noise(key_list[19], (2, SEQS, KERNEL - 1, GROUPS * STATE), 1.0, 6.0, ((1, 4), (3, 8)))
    return {"tokens": tokens, "lengths": lengths, "norm_gain": norm_gain, "w_gate": w_gate, "w_value": w_value, "w_write": w_write, "w_read": w_read, "w_step": w_step, "step_bias": step_bias, "decay_rate": decay_rate, "skip_gain": skip_gain, "conv_value_w": conv_value_w, "conv_write_w": conv_write_w, "conv_read_w": conv_read_w, "group_gain": group_gain, "w_out": w_out, "state": state, "hist_value": hist_value, "hist_write": hist_write, "hist_read": hist_read}


norm_eps = 1e-05

def conv_update(history, current, conv_taps, live_mask):
    kept_hist = history.astype(jnp.float32) * live_mask[:, :, None]
    mixed_sum = lax.optimization_barrier(jnp.sum(kept_hist * conv_taps[None, :-1, :], axis=1)) + current.astype(jnp.float32) * conv_taps[-1][None, :]
    fresh_hist = jnp.concatenate([kept_hist[:, 1:].astype(jnp.bfloat16), current[:, None, :]], axis=1)
    return (jax.nn.silu(mixed_sum), fresh_hist)

def reference(tokens, lengths, norm_gain, w_gate, w_value, w_write, w_read, w_step, step_bias, decay_rate, skip_gain, conv_value_w, conv_write_w, conv_read_w, group_gain, w_out, state, hist_value, hist_write, hist_read):
    seq_total = tokens.shape[0]
    hist_len = KERNEL - 1
    offsets = hist_len - jnp.arange(hist_len, dtype=jnp.int32)
    live_mask = (offsets[None, :] <= lengths[:, None]).astype(jnp.float32)
    per_group = HEADS // GROUPS
    current = tokens
    states_out, values_out, writes_out, reads_out = ([], [], [], [])
    for layer_idx in range(2):
        floats = current.astype(jnp.float32)
        row_scale = lax.rsqrt(lax.optimization_barrier(jnp.mean(floats * floats, axis=1)) + norm_eps)
        normed = (floats * row_scale[:, None] * norm_gain[layer_idx][None, :]).astype(jnp.bfloat16)
        gate_part = jnp.dot(normed, w_gate[layer_idx], preferred_element_type=jnp.float32).astype(jnp.bfloat16)
        value_part = jnp.dot(normed, w_value[layer_idx], preferred_element_type=jnp.float32).astype(jnp.bfloat16)
        write_part = jnp.dot(normed, w_write[layer_idx], preferred_element_type=jnp.float32).astype(jnp.bfloat16)
        read_part = jnp.dot(normed, w_read[layer_idx], preferred_element_type=jnp.float32).astype(jnp.bfloat16)
        step_raw = jnp.dot(normed, w_step[layer_idx], preferred_element_type=jnp.float32)
        value_act, value_hist = conv_update(hist_value[layer_idx], value_part, conv_value_w[layer_idx], live_mask)
        write_act, write_hist = conv_update(hist_write[layer_idx], write_part, conv_write_w[layer_idx], live_mask)
        read_act, read_hist = conv_update(hist_read[layer_idx], read_part, conv_read_w[layer_idx], live_mask)
        step_size = jax.nn.softplus(step_raw + step_bias[layer_idx][None, :])
        decay_keep = jnp.exp(-decay_rate[layer_idx][None, :] * step_size)
        write_groups = jnp.swapaxes(write_act.reshape(seq_total, STATE, GROUPS), 1, 2)
        read_groups = jnp.swapaxes(read_act.reshape(seq_total, STATE, GROUPS), 1, 2)
        write_heads = jnp.repeat(write_groups, per_group, axis=1)
        read_heads = jnp.repeat(read_groups, per_group, axis=1)
        inputs = value_act.reshape(seq_total, HEADS, HEAD_DIM)
        updated = decay_keep[:, :, None, None] * state[layer_idx] + (step_size[:, :, None] * inputs)[:, :, :, None] * write_heads[:, :, None, :]
        readout = jnp.einsum('shpn,shn->shp', updated, read_heads, precision=lax.Precision.HIGHEST) + skip_gain[layer_idx][None, :, None] * inputs
        gated_out = readout.reshape(seq_total, WIDTH) * jax.nn.silu(gate_part.astype(jnp.float32))
        grouped = gated_out.reshape(seq_total, GROUPS, WIDTH // GROUPS)
        grouped = grouped * lax.rsqrt(lax.optimization_barrier(jnp.mean(grouped * grouped, axis=2, keepdims=True)) + norm_eps)
        mixer_out = (grouped.reshape(seq_total, WIDTH) * group_gain[layer_idx][None, :]).astype(jnp.bfloat16)
        current = jnp.dot(mixer_out, w_out[layer_idx], preferred_element_type=jnp.float32)
        if layer_idx == 0:
            current = current.astype(jnp.bfloat16)
        states_out.append(updated)
        values_out.append(value_hist)
        writes_out.append(write_hist)
        reads_out.append(read_hist)
    return (current, jnp.stack(states_out), jnp.stack(values_out), jnp.stack(writes_out), jnp.stack(reads_out))
```

```python
import functools

import jax
import jax.numpy as jnp
from jax import lax
from jax.experimental import pallas as pl
from jax.experimental.pallas import tpu as pltpu
from jax.sharding import PartitionSpec as P

GROUPS = 2
norm_eps = 1e-05
MESH = pl.DeviceIdType.MESH
VMEM = pltpu.VMEM
LANES = 128
TOK, WR0, CONV, GAIN, OUT0, WR1, OUT1 = range(7)
F32 = jnp.float32
BF16 = jnp.bfloat16

NT = (((1,), (1,)), ((), ()))
NN = (((1,), (0,)), ((), ()))


def dot(a, b, dims=NN, **kw):
    return lax.dot_general(a, b, dims, preferred_element_type=F32, **kw)


def sigmoid_mul(x):
    return x * (1.0 / (1.0 + jnp.exp(-x)))


def iota(shape, axis):
    return lax.broadcasted_iota(jnp.int32, shape, axis)


def live_columns(lengths, seq, hist_len):
    row = jnp.broadcast_to(lengths.astype(F32), (seq, seq))
    same = iota((seq, seq), 0) == iota((seq, seq), 1)
    column = jnp.sum(jnp.where(same, row, 0.0), axis=1, keepdims=True)
    return [(column >= float(hist_len - k)).astype(F32) for k in range(hist_len)]


def mixer_kernel(
    tp, dp, tokens, lengths, norm_gain, w_gate, w_value, w_write, w_read, w_step,
    step_bias, decay_rate, skip_gain, tap_value, tap_write, tap_read, group_gain,
    w_out, state, hist_value, hist_write, hist_read,
    mixed, aux, fresh,
    tok_buf, wr_send, wr_buf, conv_send, conv_buf, gain_send, gain_buf, out_buf,
    local_w, cur, rs_send, rs_buf, mix_send, mix_buf, last_buf, st, stb,
    tp_send, tp_recv, rs_ssem, rs_rsem, mix_ssem, mix_rsem, last_ssem, last_rsem, st_sem,
):
    t = lax.axis_index("tp")
    d = lax.axis_index("dp")
    rows = tokens.shape[0]
    hist_len, seq, vcols = hist_value.shape[1:]
    wcols = w_write.shape[1]
    cj = wcols // GROUPS
    nstate = state.shape[-1]
    hdim = state.shape[-2]
    feats = tokens.shape[1]
    total = feats * dp
    seqs = seq * dp
    per_group = tp // GROUPS
    group = t // per_group
    k_blocks = tp // dp
    packed = mix_send.shape[1]
    lane = iota((1, LANES), 1)
    low = lane < hdim

    barrier = pltpu.get_barrier_semaphore()
    for i in range(1, tp):
        pl.semaphore_signal(barrier, inc=1, device_id={"tp": lax.rem(t + i, tp), "dp": d}, device_id_type=MESH)
    for i in range(1, dp):
        pl.semaphore_signal(barrier, inc=1, device_id={"tp": t, "dp": lax.rem(d + i, dp)}, device_id_type=MESH)
    st_copy = pltpu.make_async_copy(state, st, st_sem)
    st_copy.start()

    size = 2 * wcols
    r, c = iota((size, size), 0), iota((size, size), 1)
    source = ((r // cj) % 2) * wcols + (r % cj) * GROUPS + r // (2 * cj)
    pick = (c == source).astype(F32)
    pick16 = pick.astype(BF16)
    live = live_columns(lengths[...], seq, hist_len)
    for l in range(2):
        both = jnp.concatenate([w_write[l], w_read[l]], axis=0)
        got = dot(pick16, both).astype(BF16)
        for g in range(GROUPS):
            for kind in range(2):
                at = (g * 2 + kind) * cj
                wr_send[l, g, kind] = got[at:at + cj]

    pl.semaphore_wait(barrier, tp + dp - 2)
    sent = []

    def spread(cat, src_of, dst):
        out = []
        for i in range(1, tp):
            to = lax.rem(t + i, tp)
            copy = pltpu.make_async_remote_copy(
                src_ref=src_of(to), dst_ref=dst, send_sem=tp_send.at[cat, i - 1],
                recv_sem=tp_recv.at[cat, i - 1], device_id={"tp": to, "dp": d}, device_id_type=MESH)
            copy.start()
            out.append(copy)
        sent.extend(out)
        return out

    got_tok = spread(TOK, lambda to: tokens, tok_buf.at[t])
    got_wr = [spread(WR0, lambda to: wr_send.at[0, to // per_group], wr_buf.at[0, :, t]), None]

    pieces = []
    for l in range(2):
        parts = []
        for hist, tap in ((hist_write, tap_write), (hist_read, tap_read)):
            total_c = sum(hist[l, k].astype(F32) * live[k] * tap[l, k:k + 1] for k in range(hist_len))
            last = tap[l, hist_len:hist_len + 1]
            parts.append(jnp.concatenate([total_c, last, jnp.zeros((7, wcols), F32)], axis=0))
        pieces.append(jnp.concatenate(parts, axis=1))
    span = seq + 8
    pieces.append(jnp.zeros((LANES - 2 * span, size), F32))
    moved = dot(pick, jnp.concatenate(pieces, axis=0), NT, precision=lax.Precision.HIGHEST)
    for g in range(GROUPS):
        for kind in range(2):
            at = (g * 2 + kind) * cj
            conv_send[g, kind] = moved[at:at + cj]
    gg = group_gain[...]
    gain_send[...] = jnp.concatenate([jnp.concatenate([gg, gg], axis=1), jnp.zeros((6, LANES), F32)], axis=0)
    got_conv = spread(CONV, lambda to: conv_send.at[to // per_group], conv_buf.at[:, t])
    got_gain = spread(GAIN, lambda to: gain_send, gain_buf.at[t])
    got_out = [spread(OUT0, lambda to: w_out.at[0], out_buf.at[0, t]), None]
    got_wr[1] = spread(WR1, lambda to: wr_send.at[1, to // per_group], wr_buf.at[1, :, t])
    got_out[1] = spread(OUT1, lambda to: w_out.at[1], out_buf.at[1, t])

    tok_buf[t] = tokens[...]
    conv_buf[:, t] = conv_send[group]
    gain_buf[t] = gain_send[...]
    for l in range(2):
        wr_buf[l, :, t] = wr_send[l, group]
        out_buf[l, t] = w_out[l]
        local_w[l, 0] = jnp.concatenate([w_value[l], w_gate[l]], axis=0)
        local_w[l, 1] = jnp.concatenate(
            [w_write[l], w_read[l], w_step[l:l + 1], jnp.zeros((LANES - size - 1, feats), BF16)], axis=0)
    st_copy.wait()
    for l in range(2):
        stb[l] = st[l].reshape(seq * hdim, nstate).astype(BF16)

    for copy in got_tok:
        copy.wait_recv()
    for i in range(tp):
        cur[i * rows:(i + 1) * rows] = tok_buf[i].astype(F32)

    def pair_rows(get, p):
        a, b = get(2 * p).astype(F32), get(2 * p + 1).astype(F32)
        ra, rb = pltpu.roll(a, hdim, 1), pltpu.roll(b, hdim, 1)
        cut = 2 * packed - seq
        return jnp.concatenate([jnp.where(low, a, rb), jnp.where(low, ra, b)[cut:]], axis=0)

    def normed_rows(get, l):
        cols = [pair_rows(get, p) for p in range(tp // 2)]
        pairs = tp // 2 // GROUPS
        done = []
        for g in range(GROUPS):
            own = cols[g * pairs:(g + 1) * pairs]
            sq = sum(jnp.sum(x * x, axis=1, keepdims=True) for x in own)
            scale = lax.rsqrt(sq / (per_group * hdim) + norm_eps)
            for p, x in enumerate(own):
                at = 2 * (g * pairs + p)
                gain = jnp.where(low, gain_buf[at, l:l + 1], gain_buf[at + 1, l:l + 1])
                done.append((x * scale * gain).astype(BF16))
        return jnp.concatenate(done, axis=1)

    for l in range(2):
        value = cur[...]
        x = (value * norm_gain[l:l + 1]).astype(BF16)
        squares = jnp.sum(value * value, axis=1, keepdims=True)
        first = dot(x, local_w[l, 0], NT)
        last = dot(x, local_w[l, 1], NT)
        last = jnp.where(lane == size + 1, squares, last)
        for j in range(dp):
            rs_send[l, j, :, 0:LANES] = first[j * seq:(j + 1) * seq].astype(BF16)
            rs_send[l, j, :, 3 * LANES:] = last[j * seq:(j + 1) * seq].astype(BF16)
        for copy in got_wr[l]:
            copy.wait_recv()
        for kind in range(2):
            mid = dot(x, wr_buf[l, kind].reshape(nstate, feats), NT)
            for j in range(dp):
                rs_send[l, j, :, (1 + kind) * LANES:(2 + kind) * LANES] = mid[j * seq:(j + 1) * seq].astype(BF16)
        got = []
        for i in range(1, dp):
            to = lax.rem(d + i, dp)
            copy = pltpu.make_async_remote_copy(
                src_ref=rs_send.at[l, to], dst_ref=rs_buf.at[l, d], send_sem=rs_ssem.at[l, i - 1],
                recv_sem=rs_rsem.at[l, i - 1], device_id={"tp": t, "dp": to}, device_id_type=MESH)
            copy.start()
            got.append(copy)
        sent.extend(got)
        rs_buf[l, d] = rs_send[l, d]
        value_hist = sum(
            hist_value[l, k].astype(F32) * live[k] * tap_value[l, k:k + 1] for k in range(hist_len))
        if l == 0:
            for copy in got_conv + got_gain:
                copy.wait_recv()
            convs = [conv_buf[kind].reshape(nstate, LANES).T for kind in range(2)]
        for copy in got:
            copy.wait_recv()
        z = sum(rs_buf[l, j].astype(F32) for j in range(dp))
        z = z * lax.rsqrt(z[:, 3 * LANES + size + 1:3 * LANES + size + 2] / total + norm_eps)
        step_raw = z[:, 3 * LANES + size:3 * LANES + size + 1]
        z16 = z.astype(BF16)
        zr = z16.astype(F32)
        fresh[l, :, 0:LANES] = z16[:, 0:LANES]
        fresh[l, :, LANES:] = z16[:, 3 * LANES:]
        acts = []
        for kind in range(2):
            base = convs[kind][l * span:l * span + seq]
            tap = convs[kind][l * span + seq:l * span + seq + 1]
            acts.append(sigmoid_mul(base + tap * zr[:, (1 + kind) * LANES:(2 + kind) * LANES]))
        write, read = acts
        u = sigmoid_mul(value_hist + tap_value[l, hist_len:hist_len + 1] * zr[:, 0:vcols])
        gate = zr[:, vcols:2 * vcols]
        pre = step_raw + step_bias[0, l]
        step = jnp.maximum(pre, 0.0) + jnp.log1p(jnp.exp(-jnp.abs(pre)))
        keep = jnp.exp(-decay_rate[0, l] * step)
        read16 = read.astype(BF16)
        held = jnp.zeros((seq, 2 * hdim), F32)
        which = iota((seq, 1), 0)
        for j in range(seq // 2):
            part = dot(read16, stb[l, 2 * j * hdim:2 * (j + 1) * hdim, :], NT)
            held = jnp.where(which // 2 == j, part, held)
        held = jnp.where(which % 2 == 0, held[:, :hdim], held[:, hdim:])
        su = step * u
        overlap = jnp.sum(write * read, axis=1, keepdims=True)
        readout = keep * held + su * overlap + skip_gain[0, l] * u
        gated = readout * sigmoid_mul(gate)
        aux[l, :, 0:nstate] = write
        aux[l, :, nstate:] = jnp.concatenate([su, jnp.broadcast_to(keep, (seq, hdim))], axis=1)
        mix_send[l] = jnp.concatenate([gated[:packed], gated[seq - packed:]], axis=1).astype(BF16)
        if l == 0:
            got = []
            for j in range(dp):
                for i in range(tp):
                    if i + j == 0:
                        continue
                    copy = pltpu.make_async_remote_copy(
                        src_ref=mix_send.at[0], dst_ref=mix_buf.at[d, t],
                        send_sem=mix_ssem.at[j * tp + i - 1], recv_sem=mix_rsem.at[j * tp + i - 1],
                        device_id={"tp": lax.rem(t + i, tp), "dp": lax.rem(d + j, dp)}, device_id_type=MESH)
                    copy.start()
                    got.append(copy)
            sent.extend(got)
            mix_buf[d, t] = mix_send[0]
            for copy in got_out[0]:
                copy.wait_recv()
            for copy in got:
                copy.wait_recv()
            lhs = jnp.concatenate(
                [normed_rows(lambda i, j=j: mix_buf[j, i], 0) for j in range(dp)], axis=0)
            full = dot(lhs, out_buf[0].reshape(tp * vcols, feats))
            cur[...] = full.astype(BF16).astype(F32)

    def last_copy(j, m):
        to = k_blocks * d + m
        return to, pltpu.make_async_remote_copy(
            src_ref=mix_send.at[1], dst_ref=last_buf.at[t], send_sem=last_ssem.at[j * k_blocks + m],
            recv_sem=last_rsem.at[t], device_id={"tp": to, "dp": lax.rem(d + j, dp)}, device_id_type=MESH)

    for j in range(dp):
        for m in range(k_blocks):
            to, copy = last_copy(j, m)
            if j == 0:
                pl.when(to != t)(copy.start)
            else:
                copy.start()
    for copy in got_out[1]:
        copy.wait_recv()

    def arrived(i):
        pltpu.make_async_remote_copy(
            src_ref=mix_send.at[1], dst_ref=last_buf.at[i], send_sem=last_ssem.at[0],
            recv_sem=last_rsem.at[i], device_id={"tp": t, "dp": lax.rem(d + 1, dp)},
            device_id_type=MESH).wait_recv()

    for i in range(1, tp):
        arrived(lax.rem(t + i, tp))
    is_mine = t // k_blocks == d
    pl.when(jnp.logical_not(is_mine))(lambda: arrived(t))

    @pl.when(is_mine)
    def _():
        last_buf[t] = mix_send[1]

    full = dot(normed_rows(lambda i: last_buf[i], 1), out_buf[1].reshape(tp * vcols, feats))
    mine = full[:rows]
    for m in range(1, k_blocks):
        mine = jnp.where(t % k_blocks == m, full[m * rows:(m + 1) * rows], mine)
    mixed[...] = mine

    for copy in sent:
        copy.wait_send()
    for j in range(dp):
        for m in range(k_blocks):
            to, copy = last_copy(j, m)
            if j == 0:
                pl.when(to != t)(copy.wait_send)
            else:
                copy.wait_send()


def finish_kernel(lengths, mixed_in, aux, fresh, state, hist_value, hist_write, hist_read,
                  mixed, new_state, new_value, new_write, new_read):
    hist_len, seq, vcols = hist_value.shape[1:]
    wcols = hist_write.shape[-1]
    nstate = state.shape[-1]
    hdim = state.shape[-2]
    l = pl.program_id(0)
    live = live_columns(lengths[...], seq, hist_len)
    mixed[...] = mixed_in[...]
    edges = (
        (hist_value, new_value, 0, vcols),
        (hist_write, new_write, LANES, wcols),
        (hist_read, new_read, LANES + wcols, wcols),
    )
    for old, new, at, width in edges:
        for k in range(1, hist_len):
            new[0, k - 1] = (old[0, k].astype(F32) * live[k]).astype(BF16)
        new[0, hist_len - 1] = fresh[0, :, at:at + width]
    write = aux[0, :, 0:nstate]
    rest = aux[0, :, nstate:].T
    for s in range(seq):
        su = rest[0:hdim, s:s + 1]
        keep = rest[hdim:, s:s + 1]
        new_state[0, s] = keep * state[0, s] + su * write[s:s + 1]


def body(tp, dp, tokens, lengths, norm_gain, w_gate, w_value, w_write, w_read, w_step, step_bias,
         decay_rate, skip_gain, conv_value_w, conv_write_w, conv_read_w, group_gain, w_out, state,
         hist_value, hist_write, hist_read):
    rows, feats = tokens.shape
    seq = state.shape[1]
    hdim, nstate = state.shape[3:]
    hist_len = hist_value.shape[2]
    vcols, wcols = w_value.shape[2], w_write.shape[2]
    cj = wcols // GROUPS
    packed = 16
    lens = lengths.reshape(1, seq)
    flip = functools.partial(jnp.swapaxes, axis1=1, axis2=2)
    state4 = state.reshape(2, seq, hdim, nstate)
    hists = [flip(h) for h in (hist_value, hist_write, hist_read)]
    vspec = pl.BlockSpec(memory_space=VMEM)
    sspec = pl.BlockSpec(memory_space=pltpu.SMEM)
    aspec = pl.BlockSpec(memory_space=pl.ANY)
    dma = pltpu.SemaphoreType.DMA
    mixed, aux, fresh = pl.pallas_call(
        functools.partial(mixer_kernel, tp, dp),
        out_shape=(
            jax.ShapeDtypeStruct((rows, feats), F32),
            jax.ShapeDtypeStruct((2, seq, nstate + 2 * hdim), F32),
            jax.ShapeDtypeStruct((2, seq, 2 * LANES), BF16),
        ),
        in_specs=[vspec] * 8 + [sspec] * 3 + [vspec] * 5 + [aspec] + [vspec] * 3,
        out_specs=(vspec,) * 3,
        scratch_shapes=[
            VMEM((tp, rows, feats), BF16),
            VMEM((2, GROUPS, 2, cj, feats), BF16),
            VMEM((2, 2, tp, cj, feats), BF16),
            VMEM((GROUPS, 2, cj, LANES), F32),
            VMEM((2, tp, cj, LANES), F32),
            VMEM((8, LANES), F32),
            VMEM((tp, 8, LANES), F32),
            VMEM((2, tp, vcols, feats), BF16),
            VMEM((2, 2, LANES, feats), BF16),
            VMEM((seq * dp, feats), F32),
            VMEM((2, dp, seq, 4 * LANES), BF16),
            VMEM((2, dp, seq, 4 * LANES), BF16),
            VMEM((2, packed, LANES), BF16),
            VMEM((dp, tp, packed, LANES), BF16),
            VMEM((tp, packed, LANES), BF16),
            VMEM((2, seq, hdim, nstate), F32),
            VMEM((2, seq * hdim, nstate), BF16),
            dma((7, tp - 1)),
            dma((7, tp - 1)),
            dma((2, dp - 1)),
            dma((2, dp - 1)),
            dma((tp * dp - 1,)),
            dma((tp * dp - 1,)),
            dma((tp,)),
            dma((tp,)),
            dma,
        ],
        compiler_params=pltpu.CompilerParams(
            collective_id=0, has_side_effects=True, vmem_limit_bytes=40 * 1024 * 1024),
        name="mixer_blocks",
    )(tokens, lens, norm_gain, flip(w_gate), flip(w_value), flip(w_write), flip(w_read),
      jnp.transpose(w_step, (2, 0, 1)).reshape(2, feats), step_bias.T, decay_rate.T, skip_gain.T,
      conv_value_w, conv_write_w, conv_read_w, group_gain, w_out, state4, *hists)

    def whole(shape):
        return pl.BlockSpec(shape, lambda l: (0,) * len(shape))

    def layer(shape):
        return pl.BlockSpec((1,) + shape[1:], lambda l: (l,) + (0,) * (len(shape) - 1))

    mixed, new_state, *fresh_hists = pl.pallas_call(
        finish_kernel,
        grid=(2,),
        out_shape=(
            jax.ShapeDtypeStruct(mixed.shape, F32),
            jax.ShapeDtypeStruct(state4.shape, F32),
            *[jax.ShapeDtypeStruct(h.shape, BF16) for h in hists],
        ),
        in_specs=[whole(lens.shape), whole(mixed.shape), layer(aux.shape), layer(fresh.shape),
                  layer(state4.shape), *[layer(h.shape) for h in hists]],
        out_specs=(whole(mixed.shape), layer(state4.shape), *[layer(h.shape) for h in hists]),
        name="new_states",
    )(lens, mixed, aux, fresh, state4, *hists)
    return (mixed, new_state.reshape(state.shape), *[flip(h) for h in fresh_hists])


def solution(mesh):
    columns = P(None, "dp", "tp")
    heads = P(None, "tp")
    taps = P(None, None, "tp")
    states = P(None, "dp", "tp", None, None)
    history = P(None, "dp", None, "tp")
    in_specs = (
        P("tp", "dp"), P("dp"), P(None, "dp"), columns, columns, columns, columns, columns,
        heads, heads, heads, taps, taps, taps, heads, P(None, "tp", "dp"), states,
        history, history, history,
    )
    out_specs = (P("tp", "dp"), states, history, history, history)
    run = functools.partial(body, mesh.shape["tp"], mesh.shape["dp"])
    return jax.shard_map(run, mesh=mesh, in_specs=in_specs, out_specs=out_specs, check_vma=False)
```

```python
import functools

import jax
import jax.numpy as jnp
from jax import lax
from jax.experimental import pallas as pl
from jax.experimental.pallas import tpu as pltpu
from jax.sharding import PartitionSpec as P

GROUPS = 2
norm_eps = 1e-05
MESH = pl.DeviceIdType.MESH
VMEM = pltpu.VMEM
LANES = 128
TOK, WR0, CONV, GAIN, OUT0, WR1, OUT1 = range(7)
F32 = jnp.float32
BF16 = jnp.bfloat16

NT = (((1,), (1,)), ((), ()))
NN = (((1,), (0,)), ((), ()))


def dot(a, b, dims=NN, **kw):
    return lax.dot_general(a, b, dims, preferred_element_type=F32, **kw)


def sigmoid_mul(x):
    return x * (1.0 / (1.0 + jnp.exp(-x)))


def iota(shape, axis):
    return lax.broadcasted_iota(jnp.int32, shape, axis)


def live_columns(lengths, seq, hist_len):
    row = jnp.broadcast_to(lengths.astype(F32), (seq, seq))
    same = iota((seq, seq), 0) == iota((seq, seq), 1)
    column = jnp.sum(jnp.where(same, row, 0.0), axis=1, keepdims=True)
    return [(column >= float(hist_len - k)).astype(F32) for k in range(hist_len)]


def mixer_kernel(
    tp, dp, *refs,
):
    count = 20
    held_in = refs[:count]
    mixed_out, aux_out, fresh_out = refs[count:count + 3]
    local = refs[count + 3:2 * count + 3]
    (
        tokens, lengths, norm_gain, w_gate, w_value, w_write, w_read, w_step, step_bias,
        decay_rate, skip_gain, tap_value, tap_write, tap_read, group_gain, w_out, st,
        hist_value, hist_write, hist_read,
    ) = local
    (
    mixed, aux, fresh, in_sem, out_sem,
    tok_buf, wr_send, wr_buf, conv_send, conv_buf, gain_send, gain_buf, out_buf,
    local_w, cur, rs_send, rs_buf, mix_send, mix_buf, last_buf, stb,
    tp_send, tp_recv, rs_ssem, rs_rsem, mix_ssem, mix_rsem, last_ssem, last_rsem,
    ) = refs[2 * count + 3:]
    loads = [pltpu.make_async_copy(a, b, in_sem.at[i]) for i, (a, b) in enumerate(zip(held_in, local))]
    t = lax.axis_index("tp")
    d = lax.axis_index("dp")
    rows = tokens.shape[0]
    hist_len, seq, vcols = hist_value.shape[1:]
    wcols = w_write.shape[1]
    cj = wcols // GROUPS
    nstate = st.shape[-1]
    hdim = st.shape[-2]
    feats = tokens.shape[1]
    total = feats * dp
    seqs = seq * dp
    per_group = tp // GROUPS
    group = t // per_group
    k_blocks = tp // dp
    packed = mix_send.shape[1]
    lane = iota((1, LANES), 1)
    low = lane < hdim

    barrier = pltpu.get_barrier_semaphore()
    for i in range(1, tp):
        pl.semaphore_signal(barrier, inc=1, device_id={"tp": lax.rem(t + i, tp), "dp": d}, device_id_type=MESH)
    for i in range(1, dp):
        pl.semaphore_signal(barrier, inc=1, device_id={"tp": t, "dp": lax.rem(d + i, dp)}, device_id_type=MESH)
    early = (0, 5, 6)
    middle = (1, 11, 12, 13, 14, 17, 18, 19, 15)
    late = tuple(i for i in range(count) if i not in early + middle and i != 16)
    for i in early + middle + late + (16,):
        loads[i].start()
    for i in early:
        loads[i].wait()

    size = 2 * wcols
    r, c = iota((size, size), 0), iota((size, size), 1)
    source = ((r // cj) % 2) * wcols + (r % cj) * GROUPS + r // (2 * cj)
    pick = (c == source).astype(F32)
    pick16 = pick.astype(BF16)
    for l in range(2):
        both = jnp.concatenate([w_write[l], w_read[l]], axis=0)
        got = dot(pick16, both).astype(BF16)
        for g in range(GROUPS):
            for kind in range(2):
                at = (g * 2 + kind) * cj
                wr_send[l, g, kind] = got[at:at + cj]

    pl.semaphore_wait(barrier, tp + dp - 2)
    sent = []

    def spread(cat, src_of, dst):
        out = []
        for i in range(1, tp):
            to = lax.rem(t + i, tp)
            copy = pltpu.make_async_remote_copy(
                src_ref=src_of(to), dst_ref=dst, send_sem=tp_send.at[cat, i - 1],
                recv_sem=tp_recv.at[cat, i - 1], device_id={"tp": to, "dp": d}, device_id_type=MESH)
            copy.start()
            out.append(copy)
        sent.extend(out)
        return out

    got_tok = spread(TOK, lambda to: tokens, tok_buf.at[t])
    got_wr = [spread(WR0, lambda to: wr_send.at[0, to // per_group], wr_buf.at[0, :, t]), None]

    for i in middle:
        loads[i].wait()
    got_out = [spread(OUT0, lambda to: w_out.at[0], out_buf.at[0, t]), None]
    live = live_columns(lengths[...], seq, hist_len)
    pieces = []
    for l in range(2):
        parts = []
        for hist, tap in ((hist_write, tap_write), (hist_read, tap_read)):
            total_c = sum(hist[l, k].astype(F32) * live[k] * tap[l, k:k + 1] for k in range(hist_len))
            last = tap[l, hist_len:hist_len + 1]
            parts.append(jnp.concatenate([total_c, last, jnp.zeros((7, wcols), F32)], axis=0))
        pieces.append(jnp.concatenate(parts, axis=1))
    span = seq + 8
    pieces.append(jnp.zeros((LANES - 2 * span, size), F32))
    moved = dot(pick, jnp.concatenate(pieces, axis=0), NT, precision=lax.Precision.HIGHEST)
    for g in range(GROUPS):
        for kind in range(2):
            at = (g * 2 + kind) * cj
            conv_send[g, kind] = moved[at:at + cj]
    gg = group_gain[...]
    gain_send[...] = jnp.concatenate([jnp.concatenate([gg, gg], axis=1), jnp.zeros((6, LANES), F32)], axis=0)
    got_conv = spread(CONV, lambda to: conv_send.at[to // per_group], conv_buf.at[:, t])
    got_gain = spread(GAIN, lambda to: gain_send, gain_buf.at[t])
    got_wr[1] = spread(WR1, lambda to: wr_send.at[1, to // per_group], wr_buf.at[1, :, t])
    got_out[1] = spread(OUT1, lambda to: w_out.at[1], out_buf.at[1, t])

    for i in late:
        loads[i].wait()
    tok_buf[t] = tokens[...]
    conv_buf[:, t] = conv_send[group]
    gain_buf[t] = gain_send[...]
    for l in range(2):
        wr_buf[l, :, t] = wr_send[l, group]
        out_buf[l, t] = w_out[l]
        local_w[l, 0] = jnp.concatenate([w_value[l], w_gate[l]], axis=0)
        local_w[l, 1] = jnp.concatenate(
            [w_write[l], w_read[l], w_step[l:l + 1], jnp.zeros((LANES - size - 1, feats), BF16)], axis=0)
    loads[16].wait()
    for l in range(2):
        stb[l] = st[l].reshape(seq * hdim, nstate).astype(BF16)

    for copy in got_tok:
        copy.wait_recv()
    for i in range(tp):
        cur[i * rows:(i + 1) * rows] = tok_buf[i].astype(F32)

    def pair_rows(get, p):
        a, b = get(2 * p).astype(F32), get(2 * p + 1).astype(F32)
        ra, rb = pltpu.roll(a, hdim, 1), pltpu.roll(b, hdim, 1)
        cut = 2 * packed - seq
        return jnp.concatenate([jnp.where(low, a, rb), jnp.where(low, ra, b)[cut:]], axis=0)

    def normed_rows(get, l):
        cols = [pair_rows(get, p) for p in range(tp // 2)]
        pairs = tp // 2 // GROUPS
        done = []
        for g in range(GROUPS):
            own = cols[g * pairs:(g + 1) * pairs]
            sq = sum(jnp.sum(x * x, axis=1, keepdims=True) for x in own)
            scale = lax.rsqrt(sq / (per_group * hdim) + norm_eps)
            for p, x in enumerate(own):
                at = 2 * (g * pairs + p)
                gain = jnp.where(low, gain_buf[at, l:l + 1], gain_buf[at + 1, l:l + 1])
                done.append((x * scale * gain).astype(BF16))
        return jnp.concatenate(done, axis=1)

    stores = []
    for l in range(2):
        value = cur[...]
        x = (value * norm_gain[l:l + 1]).astype(BF16)
        squares = jnp.sum(value * value, axis=1, keepdims=True)
        first = dot(x, local_w[l, 0], NT)
        last = dot(x, local_w[l, 1], NT)
        last = jnp.where(lane == size + 1, squares, last)
        for j in range(dp):
            rs_send[l, j, :, 0:LANES] = first[j * seq:(j + 1) * seq].astype(BF16)
            rs_send[l, j, :, 3 * LANES:] = last[j * seq:(j + 1) * seq].astype(BF16)
        for copy in got_wr[l]:
            copy.wait_recv()
        for kind in range(2):
            mid = dot(x, wr_buf[l, kind].reshape(nstate, feats), NT)
            for j in range(dp):
                rs_send[l, j, :, (1 + kind) * LANES:(2 + kind) * LANES] = mid[j * seq:(j + 1) * seq].astype(BF16)
        got = []
        for i in range(1, dp):
            to = lax.rem(d + i, dp)
            copy = pltpu.make_async_remote_copy(
                src_ref=rs_send.at[l, to], dst_ref=rs_buf.at[l, d], send_sem=rs_ssem.at[l, i - 1],
                recv_sem=rs_rsem.at[l, i - 1], device_id={"tp": t, "dp": to}, device_id_type=MESH)
            copy.start()
            got.append(copy)
        sent.extend(got)
        rs_buf[l, d] = rs_send[l, d]
        value_hist = sum(
            hist_value[l, k].astype(F32) * live[k] * tap_value[l, k:k + 1] for k in range(hist_len))
        if l == 0:
            for copy in got_conv + got_gain:
                copy.wait_recv()
            convs = [conv_buf[kind].reshape(nstate, LANES).T for kind in range(2)]
        for copy in got:
            copy.wait_recv()
        z = sum(rs_buf[l, j].astype(F32) for j in range(dp))
        z = z * lax.rsqrt(z[:, 3 * LANES + size + 1:3 * LANES + size + 2] / total + norm_eps)
        step_raw = z[:, 3 * LANES + size:3 * LANES + size + 1]
        z16 = z.astype(BF16)
        zr = z16.astype(F32)
        fresh[l, :, 0:LANES] = z16[:, 0:LANES]
        fresh[l, :, LANES:] = z16[:, 3 * LANES:]
        acts = []
        for kind in range(2):
            base = convs[kind][l * span:l * span + seq]
            tap = convs[kind][l * span + seq:l * span + seq + 1]
            acts.append(sigmoid_mul(base + tap * zr[:, (1 + kind) * LANES:(2 + kind) * LANES]))
        write, read = acts
        u = sigmoid_mul(value_hist + tap_value[l, hist_len:hist_len + 1] * zr[:, 0:vcols])
        gate = zr[:, vcols:2 * vcols]
        pre = step_raw + step_bias[:, l:l + 1]
        step = jnp.maximum(pre, 0.0) + jnp.log1p(jnp.exp(-jnp.abs(pre)))
        keep = jnp.exp(-decay_rate[:, l:l + 1] * step)
        read16 = read.astype(BF16)
        held = jnp.zeros((seq, 2 * hdim), F32)
        which = iota((seq, 1), 0)
        for j in range(seq // 2):
            part = dot(read16, stb[l, 2 * j * hdim:2 * (j + 1) * hdim, :], NT)
            held = jnp.where(which // 2 == j, part, held)
        held = jnp.where(which % 2 == 0, held[:, :hdim], held[:, hdim:])
        su = step * u
        overlap = jnp.sum(write * read, axis=1, keepdims=True)
        readout = keep * held + su * overlap + skip_gain[:, l:l + 1] * u
        gated = readout * sigmoid_mul(gate)
        aux[l, :, 0:nstate] = write
        aux[l, :, nstate:] = jnp.concatenate([su, jnp.broadcast_to(keep, (seq, hdim))], axis=1)
        stores.append(pltpu.make_async_copy(aux.at[l], aux_out.at[l], out_sem.at[2 * l]))
        stores.append(pltpu.make_async_copy(fresh.at[l], fresh_out.at[l], out_sem.at[2 * l + 1]))
        mix_send[l] = jnp.concatenate([gated[:packed], gated[seq - packed:]], axis=1).astype(BF16)
        if l == 0:
            got = []
            for j in range(dp):
                for i in range(tp):
                    if i + j == 0:
                        continue
                    copy = pltpu.make_async_remote_copy(
                        src_ref=mix_send.at[0], dst_ref=mix_buf.at[d, t],
                        send_sem=mix_ssem.at[j * tp + i - 1], recv_sem=mix_rsem.at[j * tp + i - 1],
                        device_id={"tp": lax.rem(t + i, tp), "dp": lax.rem(d + j, dp)}, device_id_type=MESH)
                    copy.start()
                    got.append(copy)
            sent.extend(got)
            mix_buf[d, t] = mix_send[0]
            for copy in got_out[0]:
                copy.wait_recv()
            for copy in got:
                copy.wait_recv()
            lhs = jnp.concatenate(
                [normed_rows(lambda i, j=j: mix_buf[j, i], 0) for j in range(dp)], axis=0)
            full = dot(lhs, out_buf[0].reshape(tp * vcols, feats))
            cur[...] = full.astype(BF16).astype(F32)

    def last_copy(j, m):
        to = k_blocks * d + m
        return to, pltpu.make_async_remote_copy(
            src_ref=mix_send.at[1], dst_ref=last_buf.at[t], send_sem=last_ssem.at[j * k_blocks + m],
            recv_sem=last_rsem.at[t], device_id={"tp": to, "dp": lax.rem(d + j, dp)}, device_id_type=MESH)

    for j in range(dp):
        for m in range(k_blocks):
            to, copy = last_copy(j, m)
            if j == 0:
                pl.when(to != t)(copy.start)
            else:
                copy.start()
    for copy in stores:
        copy.start()
    for copy in got_out[1]:
        copy.wait_recv()

    def arrived(i):
        pltpu.make_async_remote_copy(
            src_ref=mix_send.at[1], dst_ref=last_buf.at[i], send_sem=last_ssem.at[0],
            recv_sem=last_rsem.at[i], device_id={"tp": t, "dp": lax.rem(d + 1, dp)},
            device_id_type=MESH).wait_recv()

    for i in range(1, tp):
        arrived(lax.rem(t + i, tp))
    is_mine = t // k_blocks == d
    pl.when(jnp.logical_not(is_mine))(lambda: arrived(t))

    @pl.when(is_mine)
    def _():
        last_buf[t] = mix_send[1]

    full = dot(normed_rows(lambda i: last_buf[i], 1), out_buf[1].reshape(tp * vcols, feats))
    mine = full[:rows]
    for m in range(1, k_blocks):
        mine = jnp.where(t % k_blocks == m, full[m * rows:(m + 1) * rows], mine)
    mixed[...] = mine
    stores.append(pltpu.make_async_copy(mixed, mixed_out, out_sem.at[4]))
    stores[-1].start()

    for copy in sent:
        copy.wait_send()
    for j in range(dp):
        for m in range(k_blocks):
            to, copy = last_copy(j, m)
            if j == 0:
                pl.when(to != t)(copy.wait_send)
            else:
                copy.wait_send()
    for copy in stores:
        copy.wait()


def finish_kernel(lengths, mixed_in, aux, fresh, state, hist_value, hist_write, hist_read,
                  mixed, new_state, new_value, new_write, new_read):
    hist_len, seq, vcols = hist_value.shape[1:]
    wcols = hist_write.shape[-1]
    nstate = state.shape[-1]
    hdim = state.shape[-2]
    first = pl.program_id(1) == 0

    @pl.when(first)
    def _():
        live = live_columns(lengths[...], seq, hist_len)
        mixed[...] = mixed_in[...]
        edges = (
            (hist_value, new_value, 0, vcols),
            (hist_write, new_write, LANES, wcols),
            (hist_read, new_read, LANES + wcols, wcols),
        )
        for old, new, at, width in edges:
            for k in range(1, hist_len):
                new[0, k - 1] = (old[0, k].astype(F32) * live[k]).astype(BF16)
            new[0, hist_len - 1] = fresh[0, :, at:at + width]

    write = aux[0, :, 0:nstate]
    rest = aux[0, :, nstate:].T
    for s in range(state.shape[1]):
        su = rest[0:hdim, s:s + 1]
        keep = rest[hdim:, s:s + 1]
        new_state[0, s] = keep * state[0, s] + su * write[s:s + 1]


def body(tp, dp, tokens, lengths, norm_gain, w_gate, w_value, w_write, w_read, w_step, step_bias,
         decay_rate, skip_gain, conv_value_w, conv_write_w, conv_read_w, group_gain, w_out, state,
         hist_value, hist_write, hist_read):
    rows, feats = tokens.shape
    seq = state.shape[1]
    hdim, nstate = state.shape[3:]
    hist_len = hist_value.shape[2]
    vcols, wcols = w_value.shape[2], w_write.shape[2]
    cj = wcols // GROUPS
    packed = 16
    chunk = 8
    lens = lengths.reshape(1, seq)
    flip = functools.partial(jnp.swapaxes, axis1=1, axis2=2)
    state4 = state.reshape(2, seq, hdim, nstate)
    hists = [flip(h) for h in (hist_value, hist_write, hist_read)]
    aspec = pl.BlockSpec(memory_space=pl.ANY)
    dma = pltpu.SemaphoreType.DMA
    operands = (
        tokens, lens, norm_gain, flip(w_gate), flip(w_value), flip(w_write), flip(w_read),
        jnp.transpose(w_step, (2, 0, 1)).reshape(2, feats), step_bias.T, decay_rate.T, skip_gain.T,
        conv_value_w, conv_write_w, conv_read_w, group_gain, w_out, state4, *hists)
    results = (
        jax.ShapeDtypeStruct((rows, feats), F32),
        jax.ShapeDtypeStruct((2, seq, nstate + 2 * hdim), F32),
        jax.ShapeDtypeStruct((2, seq, 2 * LANES), BF16),
    )
    mixed, aux, fresh = pl.pallas_call(
        functools.partial(mixer_kernel, tp, dp),
        out_shape=results,
        in_specs=[aspec] * len(operands),
        out_specs=(aspec,) * 3,
        scratch_shapes=[
            *[VMEM(x.shape, x.dtype) for x in operands],
            *[VMEM(x.shape, x.dtype) for x in results],
            dma((len(operands),)),
            dma((5,)),
            VMEM((tp, rows, feats), BF16),
            VMEM((2, GROUPS, 2, cj, feats), BF16),
            VMEM((2, 2, tp, cj, feats), BF16),
            VMEM((GROUPS, 2, cj, LANES), F32),
            VMEM((2, tp, cj, LANES), F32),
            VMEM((8, LANES), F32),
            VMEM((tp, 8, LANES), F32),
            VMEM((2, tp, vcols, feats), BF16),
            VMEM((2, 2, LANES, feats), BF16),
            VMEM((seq * dp, feats), F32),
            VMEM((2, dp, seq, 4 * LANES), BF16),
            VMEM((2, dp, seq, 4 * LANES), BF16),
            VMEM((2, packed, LANES), BF16),
            VMEM((dp, tp, packed, LANES), BF16),
            VMEM((tp, packed, LANES), BF16),
            VMEM((2, seq * hdim, nstate), BF16),
            dma((7, tp - 1)),
            dma((7, tp - 1)),
            dma((2, dp - 1)),
            dma((2, dp - 1)),
            dma((tp * dp - 1,)),
            dma((tp * dp - 1,)),
            dma((tp,)),
            dma((tp,)),
        ],
        compiler_params=pltpu.CompilerParams(
            collective_id=0, has_side_effects=True),
        name="mixer_blocks",
    )(*operands)

    def whole(shape):
        return pl.BlockSpec(shape, lambda l, c: (0,) * len(shape))

    def layer(shape):
        return pl.BlockSpec((1,) + shape[1:], lambda l, c: (l,) + (0,) * (len(shape) - 1))

    def part(shape):
        return pl.BlockSpec((1, chunk) + shape[2:], lambda l, c: (l, c) + (0,) * (len(shape) - 2))

    mixed, new_state, *fresh_hists = pl.pallas_call(
        finish_kernel,
        grid=(2, seq // chunk),
        out_shape=(
            jax.ShapeDtypeStruct(mixed.shape, F32),
            jax.ShapeDtypeStruct(state4.shape, F32),
            *[jax.ShapeDtypeStruct(h.shape, BF16) for h in hists],
        ),
        in_specs=[whole(lens.shape), whole(mixed.shape), part(aux.shape), layer(fresh.shape),
                  part(state4.shape), *[layer(h.shape) for h in hists]],
        out_specs=(whole(mixed.shape), part(state4.shape), *[layer(h.shape) for h in hists]),
        name="new_states",
    )(lens, mixed, aux, fresh, state4, *hists)
    return (mixed, new_state.reshape(state.shape), *[flip(h) for h in fresh_hists])


def solution(mesh):
    columns = P(None, "dp", "tp")
    heads = P(None, "tp")
    taps = P(None, None, "tp")
    states = P(None, "dp", "tp", None, None)
    history = P(None, "dp", None, "tp")
    in_specs = (
        P("tp", "dp"), P("dp"), P(None, "dp"), columns, columns, columns, columns, columns,
        heads, heads, heads, taps, taps, taps, heads, P(None, "tp", "dp"), states,
        history, history, history,
    )
    out_specs = (P("tp", "dp"), states, history, history, history)
    run = functools.partial(body, mesh.shape["tp"], mesh.shape["dp"])
    return jax.shard_map(run, mesh=mesh, in_specs=in_specs, out_specs=out_specs, check_vma=False)
```

```python
import functools

import jax
import jax.numpy as jnp
from jax import lax
from jax.experimental import pallas as pl
from jax.experimental.pallas import tpu as pltpu
from jax.sharding import PartitionSpec as P

GROUPS = 2
norm_eps = 1e-05
MESH = pl.DeviceIdType.MESH
VMEM = pltpu.VMEM
LANES = 128
TOK, WR0, CONV, GAIN, OUT0, WR1, OUT1 = range(7)
F32 = jnp.float32
BF16 = jnp.bfloat16

NT = (((1,), (1,)), ((), ()))
NN = (((1,), (0,)), ((), ()))


def dot(a, b, dims=NN, **kw):
    return lax.dot_general(a, b, dims, preferred_element_type=F32, **kw)


def sigmoid_mul(x):
    return x * (1.0 / (1.0 + jnp.exp(-x)))


def iota(shape, axis):
    return lax.broadcasted_iota(jnp.int32, shape, axis)


def live_columns(lengths, seq, hist_len):
    row = jnp.broadcast_to(lengths.astype(F32), (seq, seq))
    same = iota((seq, seq), 0) == iota((seq, seq), 1)
    column = jnp.sum(jnp.where(same, row, 0.0), axis=1, keepdims=True)
    return [(column >= float(hist_len - k)).astype(F32) for k in range(hist_len)]


def mixer_kernel(
    tp, dp, *refs,
):
    count = 20
    held_in = refs[:count]
    mixed_out, aux_out, fresh_out = refs[count:count + 3]
    local = refs[count + 3:2 * count + 3]
    (
        tokens, lengths, norm_gain, w_gate, w_value, w_write, w_read, w_step, step_bias,
        decay_rate, skip_gain, tap_value, tap_write, tap_read, group_gain, w_out, st,
        hist_value, hist_write, hist_read,
    ) = local
    (
    mixed, aux, fresh, in_sem, out_sem,
    tok_buf, wr_send, wr_buf, conv_send, conv_buf, gain_send, gain_buf, out_buf,
    local_w, cur, rs_send, rs_buf, mix_send, mix_buf, last_buf, stb,
    tp_send, tp_recv, rs_ssem, rs_rsem, mix_ssem, mix_rsem, last_ssem, last_rsem,
    ) = refs[2 * count + 3:]
    loads = [pltpu.make_async_copy(a, b, in_sem.at[i]) for i, (a, b) in enumerate(zip(held_in, local))]
    t = lax.axis_index("tp")
    d = lax.axis_index("dp")
    rows = tokens.shape[0]
    hist_len, seq, vcols = hist_value.shape[1:]
    wcols = w_write.shape[1]
    cj = wcols // GROUPS
    nstate = st.shape[-1]
    hdim = st.shape[-2]
    feats = tokens.shape[1]
    total = feats * dp
    seqs = seq * dp
    per_group = tp // GROUPS
    group = t // per_group
    k_blocks = tp // dp
    packed = mix_send.shape[1]
    lane = iota((1, LANES), 1)
    low = lane < hdim

    barrier = pltpu.get_barrier_semaphore()
    for i in range(1, tp):
        pl.semaphore_signal(barrier, inc=1, device_id={"tp": lax.rem(t + i, tp), "dp": d}, device_id_type=MESH)
    for i in range(1, dp):
        pl.semaphore_signal(barrier, inc=1, device_id={"tp": t, "dp": lax.rem(d + i, dp)}, device_id_type=MESH)
    early = (0, 5, 6)
    middle = (1, 11, 12, 13, 14, 17, 18, 19, 15)
    late = tuple(i for i in range(count) if i not in early + middle and i != 16)
    for i in early + middle + late + (16,):
        loads[i].start()
    for i in early:
        loads[i].wait()

    size = 2 * wcols
    r, c = iota((size, size), 0), iota((size, size), 1)
    source = ((r // cj) % 2) * wcols + (r % cj) * GROUPS + r // (2 * cj)
    pick = (c == source).astype(F32)
    pick16 = pick.astype(BF16)
    for l in range(2):
        both = jnp.concatenate([w_write[l], w_read[l]], axis=0)
        got = dot(pick16, both).astype(BF16)
        for g in range(GROUPS):
            for kind in range(2):
                at = (g * 2 + kind) * cj
                wr_send[l, g, kind] = got[at:at + cj]

    pl.semaphore_wait(barrier, tp + dp - 2)
    sent = []

    def spread(cat, src_of, dst):
        out = []
        for i in range(1, tp):
            to = lax.rem(t + i, tp)
            copy = pltpu.make_async_remote_copy(
                src_ref=src_of(to), dst_ref=dst, send_sem=tp_send.at[cat, i - 1],
                recv_sem=tp_recv.at[cat, i - 1], device_id={"tp": to, "dp": d}, device_id_type=MESH)
            copy.start()
            out.append(copy)
        sent.extend(out)
        return out

    got_tok = spread(TOK, lambda to: tokens, tok_buf.at[t])
    got_wr = [spread(WR0, lambda to: wr_send.at[0, to // per_group], wr_buf.at[0, :, t]), []]
    got_out = [[], []]

    def flipped(index, bit):
        return index + bit * (1 - 2 * ((index // bit) % 2))

    def hop(cat, n):
        bit = tp >> (n + 1)
        to = flipped(t, bit)
        held = [t]
        for m in range(n):
            held = held + [flipped(h, tp >> (m + 1)) for h in held]
        out = []
        for i, h in enumerate(held):
            if cat == WR1:
                src = wr_send.at[1, 1 - group] if n == 0 else wr_buf.at[1, :, h]
                dst = wr_buf.at[1, :, h]
            else:
                src = dst = out_buf.at[0 if cat == OUT0 else 1, h]
            copy = pltpu.make_async_remote_copy(
                src_ref=src, dst_ref=dst, send_sem=tp_send.at[cat, (1 << n) - 1 + i],
                recv_sem=tp_recv.at[cat, (1 << n) - 1 + i], device_id={"tp": to, "dp": d}, device_id_type=MESH)
            copy.start()
            out.append(copy)
        sent.extend(out)
        return out

    rounds = tp.bit_length() - 1

    def middle_hops(cat, got):
        for n in range(1, rounds - 1):
            for copy in got:
                copy.wait_recv()
            got = hop(cat, n)
        return got

    def last_hop(cat, got):
        for copy in got:
            copy.wait_recv()
        return hop(cat, rounds - 1)


    for i in middle:
        loads[i].wait()
    live = live_columns(lengths[...], seq, hist_len)
    pieces = []
    for l in range(2):
        parts = []
        for hist, tap in ((hist_write, tap_write), (hist_read, tap_read)):
            total_c = sum(hist[l, k].astype(F32) * live[k] * tap[l, k:k + 1] for k in range(hist_len))
            last = tap[l, hist_len:hist_len + 1]
            parts.append(jnp.concatenate([total_c, last, jnp.zeros((7, wcols), F32)], axis=0))
        pieces.append(jnp.concatenate(parts, axis=1))
    span = seq + 8
    pieces.append(jnp.zeros((LANES - 2 * span, size), F32))
    moved = dot(pick, jnp.concatenate(pieces, axis=0), NT, precision=lax.Precision.HIGHEST)
    for g in range(GROUPS):
        for kind in range(2):
            at = (g * 2 + kind) * cj
            conv_send[g, kind] = moved[at:at + cj].astype(BF16)
    gg = group_gain[...]
    gain_send[...] = jnp.concatenate([gg, gg], axis=1)
    got_conv = spread(CONV, lambda to: conv_send.at[to // per_group], conv_buf.at[:, t])
    got_gain = spread(GAIN, lambda to: gain_send, gain_buf.at[t])

    for i in late:
        loads[i].wait()
    tok_buf[t] = tokens[...]
    conv_buf[:, t] = conv_send[group]
    gain_buf[t] = gain_send[...]
    for l in range(2):
        wr_buf[l, :, t] = wr_send[l, group]
        out_buf[l, t] = w_out[l]
        local_w[l, 0] = jnp.concatenate([w_value[l], w_gate[l]], axis=0)
        local_w[l, 1] = jnp.concatenate(
            [w_write[l], w_read[l], w_step[l:l + 1], jnp.zeros((LANES - size - 1, feats), BF16)], axis=0)
    loads[16].wait()
    for l in range(2):
        stb[l] = st[l].reshape(seq * hdim, nstate).astype(BF16)

    for copy in got_tok:
        copy.wait_recv()
    for i in range(tp):
        cur[i * rows:(i + 1) * rows] = tok_buf[i].astype(F32)

    def pair_rows(get, p):
        a, b = get(2 * p).astype(F32), get(2 * p + 1).astype(F32)
        ra, rb = pltpu.roll(a, hdim, 1), pltpu.roll(b, hdim, 1)
        cut = 2 * packed - seq
        return jnp.concatenate([jnp.where(low, a, rb), jnp.where(low, ra, b)[cut:]], axis=0)

    def normed_rows(get, l):
        cols = [pair_rows(get, p) for p in range(tp // 2)]
        pairs = tp // 2 // GROUPS
        done = []
        for g in range(GROUPS):
            own = cols[g * pairs:(g + 1) * pairs]
            sq = sum(jnp.sum(x * x, axis=1, keepdims=True) for x in own)
            scale = lax.rsqrt(sq / (per_group * hdim) + norm_eps)
            for p, x in enumerate(own):
                at = 2 * (g * pairs + p)
                gain = jnp.where(low, gain_buf[at, l:l + 1], gain_buf[at + 1, l:l + 1])
                done.append((x * scale * gain).astype(BF16))
        return jnp.concatenate(done, axis=1)

    stores = []
    for l in range(2):
        value = cur[...]
        x = (value * norm_gain[l:l + 1]).astype(BF16)
        squares = jnp.sum(value * value, axis=1, keepdims=True)
        first = dot(x, local_w[l, 0], NT)
        last = dot(x, local_w[l, 1], NT)
        last = jnp.where(lane == size + 1, squares, last)
        for j in range(dp):
            rs_send[l, j, :, 0:LANES] = first[j * seq:(j + 1) * seq].astype(BF16)
            rs_send[l, j, :, 3 * LANES:] = last[j * seq:(j + 1) * seq].astype(BF16)
        for copy in got_wr[l]:
            copy.wait_recv()
        for kind in range(2):
            mid = dot(x, wr_buf[l, kind].reshape(nstate, feats), NT)
            for j in range(dp):
                rs_send[l, j, :, (1 + kind) * LANES:(2 + kind) * LANES] = mid[j * seq:(j + 1) * seq].astype(BF16)
        got = []
        for i in range(1, dp):
            to = lax.rem(d + i, dp)
            copy = pltpu.make_async_remote_copy(
                src_ref=rs_send.at[l, to], dst_ref=rs_buf.at[l, d], send_sem=rs_ssem.at[l, i - 1],
                recv_sem=rs_rsem.at[l, i - 1], device_id={"tp": t, "dp": to}, device_id_type=MESH)
            copy.start()
            got.append(copy)
        sent.extend(got)
        if l == 0:
            bulk = {cat: hop(cat, 0) for cat in (WR1, OUT0, OUT1)}
        else:
            got_out[1] = last_hop(OUT1, bulk[OUT1])
        rs_buf[l, d] = rs_send[l, d]
        value_hist = sum(
            hist_value[l, k].astype(F32) * live[k] * tap_value[l, k:k + 1] for k in range(hist_len))
        if l == 0:
            for copy in got_conv + got_gain:
                copy.wait_recv()
            convs = [conv_buf[kind].reshape(nstate, LANES).astype(F32).T for kind in range(2)]
        for copy in got:
            copy.wait_recv()
        if l == 0:
            bulk = {cat: middle_hops(cat, bulk[cat]) for cat in (WR1, OUT0, OUT1)}
        z = sum(rs_buf[l, j].astype(F32) for j in range(dp))
        z = z * lax.rsqrt(z[:, 3 * LANES + size + 1:3 * LANES + size + 2] / total + norm_eps)
        step_raw = z[:, 3 * LANES + size:3 * LANES + size + 1]
        z16 = z.astype(BF16)
        zr = z16.astype(F32)
        fresh[l, :, 0:LANES] = z16[:, 0:LANES]
        fresh[l, :, LANES:] = z16[:, 3 * LANES:]
        acts = []
        for kind in range(2):
            base = convs[kind][l * span:l * span + seq]
            tap = convs[kind][l * span + seq:l * span + seq + 1]
            acts.append(sigmoid_mul(base + tap * zr[:, (1 + kind) * LANES:(2 + kind) * LANES]))
        write, read = acts
        u = sigmoid_mul(value_hist + tap_value[l, hist_len:hist_len + 1] * zr[:, 0:vcols])
        gate = zr[:, vcols:2 * vcols]
        pre = step_raw + step_bias[:, l:l + 1]
        step = jnp.maximum(pre, 0.0) + jnp.log1p(jnp.exp(-jnp.abs(pre)))
        keep = jnp.exp(-decay_rate[:, l:l + 1] * step)
        read16 = read.astype(BF16)
        held = jnp.zeros((seq, 2 * hdim), F32)
        which = iota((seq, 1), 0)
        for j in range(seq // 2):
            part = dot(read16, stb[l, 2 * j * hdim:2 * (j + 1) * hdim, :], NT)
            held = jnp.where(which // 2 == j, part, held)
        held = jnp.where(which % 2 == 0, held[:, :hdim], held[:, hdim:])
        su = step * u
        overlap = jnp.sum(write * read, axis=1, keepdims=True)
        readout = keep * held + su * overlap + skip_gain[:, l:l + 1] * u
        gated = readout * sigmoid_mul(gate)
        aux[l, :, 0:nstate] = write
        aux[l, :, nstate:] = jnp.concatenate([su, jnp.broadcast_to(keep, (seq, hdim))], axis=1)
        stores.append(pltpu.make_async_copy(aux.at[l], aux_out.at[l], out_sem.at[2 * l]))
        stores.append(pltpu.make_async_copy(fresh.at[l], fresh_out.at[l], out_sem.at[2 * l + 1]))
        mix_send[l] = jnp.concatenate([gated[:packed], gated[seq - packed:]], axis=1).astype(BF16)
        if l == 0:
            got = []
            for j in range(dp):
                for i in range(tp):
                    if i + j == 0:
                        continue
                    copy = pltpu.make_async_remote_copy(
                        src_ref=mix_send.at[0], dst_ref=mix_buf.at[d, t],
                        send_sem=mix_ssem.at[j * tp + i - 1], recv_sem=mix_rsem.at[j * tp + i - 1],
                        device_id={"tp": lax.rem(t + i, tp), "dp": lax.rem(d + j, dp)}, device_id_type=MESH)
                    copy.start()
                    got.append(copy)
            sent.extend(got)
            mix_buf[d, t] = mix_send[0]
            got_out[0] = last_hop(OUT0, bulk[OUT0])
            got_wr[1] = last_hop(WR1, bulk[WR1])
            for copy in got_out[0]:
                copy.wait_recv()
            for copy in got:
                copy.wait_recv()
            lhs = jnp.concatenate(
                [normed_rows(lambda i, j=j: mix_buf[j, i], 0) for j in range(dp)], axis=0)
            full = dot(lhs, out_buf[0].reshape(tp * vcols, feats))
            cur[...] = full.astype(BF16).astype(F32)

    def last_copy(j, m):
        to = k_blocks * d + m
        return to, pltpu.make_async_remote_copy(
            src_ref=mix_send.at[1], dst_ref=last_buf.at[t], send_sem=last_ssem.at[j * k_blocks + m],
            recv_sem=last_rsem.at[t], device_id={"tp": to, "dp": lax.rem(d + j, dp)}, device_id_type=MESH)

    for j in range(dp):
        for m in range(k_blocks):
            to, copy = last_copy(j, m)
            if j == 0:
                pl.when(to != t)(copy.start)
            else:
                copy.start()
    for copy in stores:
        copy.start()
    for copy in got_out[1]:
        copy.wait_recv()

    def arrived(i):
        pltpu.make_async_remote_copy(
            src_ref=mix_send.at[1], dst_ref=last_buf.at[i], send_sem=last_ssem.at[0],
            recv_sem=last_rsem.at[i], device_id={"tp": t, "dp": lax.rem(d + 1, dp)},
            device_id_type=MESH).wait_recv()

    for i in range(1, tp):
        arrived(lax.rem(t + i, tp))
    is_mine = t // k_blocks == d
    pl.when(jnp.logical_not(is_mine))(lambda: arrived(t))

    @pl.when(is_mine)
    def _():
        last_buf[t] = mix_send[1]

    full = dot(normed_rows(lambda i: last_buf[i], 1), out_buf[1].reshape(tp * vcols, feats))
    mine = full[:rows]
    for m in range(1, k_blocks):
        mine = jnp.where(t % k_blocks == m, full[m * rows:(m + 1) * rows], mine)
    mixed[...] = mine
    stores.append(pltpu.make_async_copy(mixed, mixed_out, out_sem.at[4]))
    stores[-1].start()

    for copy in sent:
        copy.wait_send()
    for j in range(dp):
        for m in range(k_blocks):
            to, copy = last_copy(j, m)
            if j == 0:
                pl.when(to != t)(copy.wait_send)
            else:
                copy.wait_send()
    for copy in stores:
        copy.wait()


def finish_kernel(chunk, *refs):
    ins, outs, held, made = refs[:8], refs[8:13], refs[13:21], refs[21:26]
    in_sem, st_sem, out_sem, new_sem = refs[26:]
    lengths, mixed_in, aux, fresh, state, hist_value, hist_write, hist_read = held
    mixed, new_state, new_value, new_write, new_read = made
    hist_len, seq, vcols = hist_value.shape[1:]
    wcols = hist_write.shape[-1]
    nstate = state.shape[-1]
    hdim = state.shape[-2]
    places = [(l, at) for l in range(2) for at in range(0, seq, chunk)]
    small = [i for i in range(8) if i != 4]
    loads = {i: pltpu.make_async_copy(ins[i], held[i], in_sem.at[i]) for i in small}
    blocks = []
    stores = []
    loads[2].start()
    for n, (l, at) in enumerate(places):
        blocks.append(pltpu.make_async_copy(
            ins[4].at[l, at:at + chunk], state.at[l, at:at + chunk], st_sem.at[n]))
        blocks[-1].start()
    for i in small:
        if i != 2:
            loads[i].start()
    loads[2].wait()
    for n, (l, at) in enumerate(places):
        write = aux[l, at:at + chunk, 0:nstate]
        rest = aux[l, at:at + chunk, nstate:].T
        blocks[n].wait()
        for s in range(chunk):
            su = rest[0:hdim, s:s + 1]
            keep = rest[hdim:, s:s + 1]
            new_state[l, at + s] = keep * state[l, at + s] + su * write[s:s + 1]
        stores.append(pltpu.make_async_copy(
            new_state.at[l, at:at + chunk], outs[1].at[l, at:at + chunk], new_sem.at[n]))
        stores[-1].start()
        if n == 0:
            for i in small:
                if i != 2:
                    loads[i].wait()
            live = live_columns(lengths[...], seq, hist_len)
            mixed[...] = mixed_in[...]
            edges = (
                (hist_value, new_value, 0, vcols),
                (hist_write, new_write, LANES, wcols),
                (hist_read, new_read, LANES + wcols, wcols),
            )
            for old, new, edge, width in edges:
                for m in range(2):
                    for k in range(1, hist_len):
                        new[m, k - 1] = (old[m, k].astype(F32) * live[k]).astype(BF16)
                    new[m, hist_len - 1] = fresh[m, :, edge:edge + width]
            for i in (0, 2, 3, 4):
                stores.append(pltpu.make_async_copy(made[i], outs[i], out_sem.at[i]))
                stores[-1].start()
    for copy in stores:
        copy.wait()


def body(tp, dp, tokens, lengths, norm_gain, w_gate, w_value, w_write, w_read, w_step, step_bias,
         decay_rate, skip_gain, conv_value_w, conv_write_w, conv_read_w, group_gain, w_out, state,
         hist_value, hist_write, hist_read):
    rows, feats = tokens.shape
    seq = state.shape[1]
    hdim, nstate = state.shape[3:]
    hist_len = hist_value.shape[2]
    vcols, wcols = w_value.shape[2], w_write.shape[2]
    cj = wcols // GROUPS
    packed = 16
    chunk = 8
    lens = lengths.reshape(1, seq)
    flip = functools.partial(jnp.swapaxes, axis1=1, axis2=2)
    state4 = state.reshape(2, seq, hdim, nstate)
    hists = [flip(h) for h in (hist_value, hist_write, hist_read)]
    aspec = pl.BlockSpec(memory_space=pl.ANY)
    dma = pltpu.SemaphoreType.DMA
    operands = (
        tokens, lens, norm_gain, flip(w_gate), flip(w_value), flip(w_write), flip(w_read),
        jnp.transpose(w_step, (2, 0, 1)).reshape(2, feats), step_bias.T, decay_rate.T, skip_gain.T,
        conv_value_w, conv_write_w, conv_read_w, group_gain, w_out, state4, *hists)
    results = (
        jax.ShapeDtypeStruct((rows, feats), F32),
        jax.ShapeDtypeStruct((2, seq, nstate + 2 * hdim), F32),
        jax.ShapeDtypeStruct((2, seq, 2 * LANES), BF16),
    )
    mixed, aux, fresh = pl.pallas_call(
        functools.partial(mixer_kernel, tp, dp),
        out_shape=results,
        in_specs=[aspec] * len(operands),
        out_specs=(aspec,) * 3,
        scratch_shapes=[
            *[VMEM(x.shape, x.dtype) for x in operands],
            *[VMEM(x.shape, x.dtype) for x in results],
            dma((len(operands),)),
            dma((5,)),
            VMEM((tp, rows, feats), BF16),
            VMEM((2, GROUPS, 2, cj, feats), BF16),
            VMEM((2, 2, tp, cj, feats), BF16),
            VMEM((GROUPS, 2, cj, LANES), BF16),
            VMEM((2, tp, cj, LANES), BF16),
            VMEM((2, LANES), F32),
            VMEM((tp, 2, LANES), F32),
            VMEM((2, tp, vcols, feats), BF16),
            VMEM((2, 2, LANES, feats), BF16),
            VMEM((seq * dp, feats), F32),
            VMEM((2, dp, seq, 4 * LANES), BF16),
            VMEM((2, dp, seq, 4 * LANES), BF16),
            VMEM((2, packed, LANES), BF16),
            VMEM((dp, tp, packed, LANES), BF16),
            VMEM((tp, packed, LANES), BF16),
            VMEM((2, seq * hdim, nstate), BF16),
            dma((7, tp - 1)),
            dma((7, tp - 1)),
            dma((2, dp - 1)),
            dma((2, dp - 1)),
            dma((tp * dp - 1,)),
            dma((tp * dp - 1,)),
            dma((tp,)),
            dma((tp,)),
        ],
        compiler_params=pltpu.CompilerParams(
            collective_id=0, has_side_effects=True),
        name="mixer_blocks",
    )(*operands)

    given = (lens, mixed, aux, fresh, state4, *hists)
    final = (
        jax.ShapeDtypeStruct(mixed.shape, F32),
        jax.ShapeDtypeStruct(state4.shape, F32),
        *[jax.ShapeDtypeStruct(h.shape, BF16) for h in hists],
    )
    pieces = 2 * (seq // chunk)
    mixed, new_state, *fresh_hists = pl.pallas_call(
        functools.partial(finish_kernel, chunk),
        out_shape=final,
        in_specs=[aspec] * len(given),
        out_specs=(aspec,) * len(final),
        scratch_shapes=[
            *[VMEM(x.shape, x.dtype) for x in given + final],
            dma((len(given),)),
            dma((pieces,)),
            dma((len(final),)),
            dma((pieces,)),
        ],
        name="new_states",
    )(*given)
    return (mixed, new_state.reshape(state.shape), *[flip(h) for h in fresh_hists])


def solution(mesh):
    columns = P(None, "dp", "tp")
    heads = P(None, "tp")
    taps = P(None, None, "tp")
    states = P(None, "dp", "tp", None, None)
    history = P(None, "dp", None, "tp")
    in_specs = (
        P("tp", "dp"), P("dp"), P(None, "dp"), columns, columns, columns, columns, columns,
        heads, heads, heads, taps, taps, taps, heads, P(None, "tp", "dp"), states,
        history, history, history,
    )
    out_specs = (P("tp", "dp"), states, history, history, history)
    run = functools.partial(body, mesh.shape["tp"], mesh.shape["dp"])
    return jax.shard_map(run, mesh=mesh, in_specs=in_specs, out_specs=out_specs, check_vma=False)
```

```python
import functools

import jax
import jax.numpy as jnp
from jax import lax
from jax.experimental import pallas as pl
from jax.experimental.pallas import tpu as pltpu
from jax.sharding import PartitionSpec as P

GROUPS = 2
norm_eps = 1e-05
MESH = pl.DeviceIdType.MESH
VMEM = pltpu.VMEM
LANES = 128
TOK, WR0, CONV, GAIN, OUT0, WR1, OUT1 = range(7)
F32 = jnp.float32
BF16 = jnp.bfloat16

NT = (((1,), (1,)), ((), ()))
NN = (((1,), (0,)), ((), ()))


def dot(a, b, dims=NN, **kw):
    return lax.dot_general(a, b, dims, preferred_element_type=F32, **kw)


def sigmoid_mul(x):
    return x * (1.0 / (1.0 + jnp.exp(-x)))


def iota(shape, axis):
    return lax.broadcasted_iota(jnp.int32, shape, axis)


def live_columns(lengths, seq, hist_len):
    row = jnp.broadcast_to(lengths.astype(F32), (seq, seq))
    same = iota((seq, seq), 0) == iota((seq, seq), 1)
    column = jnp.sum(jnp.where(same, row, 0.0), axis=1, keepdims=True)
    return [(column >= float(hist_len - k)).astype(F32) for k in range(hist_len)]


def mixer_kernel(
    tp, dp, *refs,
):
    count = 20
    held_in = refs[:count]
    mixed_out, aux_out, fresh_out = refs[count:count + 3]
    local = refs[count + 3:2 * count + 3]
    (
        tokens, lengths, norm_gain, w_gate, w_value, w_write, w_read, w_step, step_bias,
        decay_rate, skip_gain, tap_value, tap_write, tap_read, group_gain, w_out, st,
        hist_value, hist_write, hist_read,
    ) = local
    (
    mixed, aux, fresh, in_sem, out_sem,
    tok_buf, wr_send, wr_buf, conv_send, conv_buf, gain_send, gain_buf, out_buf,
    local_w, cur, rs_send, rs_buf, mix_send, mix_buf, last_buf, stb,
    tp_send, tp_recv, rs_ssem, rs_rsem, mix_ssem, mix_rsem, last_ssem, last_rsem,
    ) = refs[2 * count + 3:]
    loads = [pltpu.make_async_copy(a, b, in_sem.at[i]) for i, (a, b) in enumerate(zip(held_in, local))]
    t = lax.axis_index("tp")
    d = lax.axis_index("dp")
    rows = tokens.shape[0]
    hist_len, seq, vcols = hist_value.shape[1:]
    wcols = w_write.shape[1]
    cj = wcols // GROUPS
    nstate = st.shape[-1]
    hdim = st.shape[-2]
    feats = tokens.shape[1]
    total = feats * dp
    seqs = seq * dp
    per_group = tp // GROUPS
    group = t // per_group
    k_blocks = tp // dp
    packed = mix_send.shape[1]
    lane = iota((1, LANES), 1)
    low = lane < hdim

    barrier = pltpu.get_barrier_semaphore()
    for i in range(1, tp):
        pl.semaphore_signal(barrier, inc=1, device_id={"tp": lax.rem(t + i, tp), "dp": d}, device_id_type=MESH)
    for i in range(1, dp):
        pl.semaphore_signal(barrier, inc=1, device_id={"tp": t, "dp": lax.rem(d + i, dp)}, device_id_type=MESH)
    early = (0, 5, 6)
    middle = (1, 11, 12, 13, 14, 17, 18, 19, 15)
    late = tuple(i for i in range(count) if i not in early + middle and i != 16)
    for i in early + middle + late + (16,):
        loads[i].start()
    for i in early:
        loads[i].wait()

    size = 2 * wcols
    r, c = iota((size, size), 0), iota((size, size), 1)
    source = ((r // cj) % 2) * wcols + (r % cj) * GROUPS + r // (2 * cj)
    pick = (c == source).astype(F32)
    pick16 = pick.astype(BF16)
    for l in range(2):
        both = jnp.concatenate([w_write[l], w_read[l]], axis=0)
        got = dot(pick16, both).astype(BF16)
        for g in range(GROUPS):
            for kind in range(2):
                at = (g * 2 + kind) * cj
                wr_send[l, g, kind] = got[at:at + cj]

    pl.semaphore_wait(barrier, tp + dp - 2)
    sent = []

    def spread(cat, src_of, dst):
        out = []
        for i in range(1, tp):
            to = lax.rem(t + i, tp)
            copy = pltpu.make_async_remote_copy(
                src_ref=src_of(to), dst_ref=dst, send_sem=tp_send.at[cat, i - 1],
                recv_sem=tp_recv.at[cat, i - 1], device_id={"tp": to, "dp": d}, device_id_type=MESH)
            copy.start()
            out.append(copy)
        sent.extend(out)
        return out

    got_tok = spread(TOK, lambda to: tokens, tok_buf.at[t])
    got_wr = [spread(WR0, lambda to: wr_send.at[0, to // per_group], wr_buf.at[0, :, t]), []]
    got_out = [[], []]

    def flipped(index, bit):
        return index + bit * (1 - 2 * ((index // bit) % 2))

    def hop(cat, n):
        bit = tp >> (n + 1)
        to = flipped(t, bit)
        held = [t]
        for m in range(n):
            held = held + [flipped(h, tp >> (m + 1)) for h in held]
        out = []
        for i, h in enumerate(held):
            if cat == WR1:
                src = wr_send.at[1, 1 - group] if n == 0 else wr_buf.at[1, :, h]
                dst = wr_buf.at[1, :, h]
            else:
                layer = 0 if cat == OUT0 else 1
                dst = out_buf.at[layer, h]
                src = w_out.at[layer] if n == 0 else dst
            copy = pltpu.make_async_remote_copy(
                src_ref=src, dst_ref=dst, send_sem=tp_send.at[cat, (1 << n) - 1 + i],
                recv_sem=tp_recv.at[cat, (1 << n) - 1 + i], device_id={"tp": to, "dp": d}, device_id_type=MESH)
            copy.start()
            out.append(copy)
        sent.extend(out)
        return out

    rounds = tp.bit_length() - 1

    def middle_hops(cat, got):
        for n in range(1, rounds - 1):
            for copy in got:
                copy.wait_recv()
            got = hop(cat, n)
        return got

    def last_hop(cat, got):
        for copy in got:
            copy.wait_recv()
        return hop(cat, rounds - 1)


    for i in middle:
        loads[i].wait()
    live = live_columns(lengths[...], seq, hist_len)
    pieces = []
    for l in range(2):
        parts = []
        for hist, tap in ((hist_write, tap_write), (hist_read, tap_read)):
            total_c = sum(hist[l, k].astype(F32) * live[k] * tap[l, k:k + 1] for k in range(hist_len))
            last = tap[l, hist_len:hist_len + 1]
            parts.append(jnp.concatenate([total_c, last, jnp.zeros((7, wcols), F32)], axis=0))
        pieces.append(jnp.concatenate(parts, axis=1))
    span = seq + 8
    pieces.append(jnp.zeros((LANES - 2 * span, size), F32))
    moved = dot(pick, jnp.concatenate(pieces, axis=0), NT, precision=lax.Precision.HIGHEST)
    for g in range(GROUPS):
        for kind in range(2):
            at = (g * 2 + kind) * cj
            conv_send[g, kind] = moved[at:at + cj].astype(BF16)
    gg = group_gain[...]
    gain_send[...] = jnp.concatenate([gg, gg], axis=1)
    got_conv = spread(CONV, lambda to: conv_send.at[to // per_group], conv_buf.at[:, t])
    got_gain = spread(GAIN, lambda to: gain_send, gain_buf.at[t])

    bulk = {OUT0: hop(OUT0, 0)}
    for i in late:
        loads[i].wait()
    tok_buf[t] = tokens[...]
    conv_buf[:, t] = conv_send[group]
    gain_buf[t] = gain_send[...]
    for l in range(2):
        wr_buf[l, :, t] = wr_send[l, group]
        out_buf[l, t] = w_out[l]
        local_w[l, 0] = jnp.concatenate([w_value[l], w_gate[l]], axis=0)
        local_w[l, 1] = jnp.concatenate(
            [w_write[l], w_read[l], w_step[l:l + 1], jnp.zeros((LANES - size - 1, feats), BF16)], axis=0)
    loads[16].wait()
    for l in range(2):
        stb[l] = st[l].reshape(seq * hdim, nstate).astype(BF16)

    for copy in got_tok:
        copy.wait_recv()
    for i in range(tp):
        cur[i * rows:(i + 1) * rows] = tok_buf[i].astype(F32)

    def pair_rows(get, p):
        a, b = get(2 * p).astype(F32), get(2 * p + 1).astype(F32)
        ra, rb = pltpu.roll(a, hdim, 1), pltpu.roll(b, hdim, 1)
        cut = 2 * packed - seq
        return jnp.concatenate([jnp.where(low, a, rb), jnp.where(low, ra, b)[cut:]], axis=0)

    def normed_rows(get, l):
        cols = [pair_rows(get, p) for p in range(tp // 2)]
        pairs = tp // 2 // GROUPS
        done = []
        for g in range(GROUPS):
            own = cols[g * pairs:(g + 1) * pairs]
            sq = sum(jnp.sum(x * x, axis=1, keepdims=True) for x in own)
            scale = lax.rsqrt(sq / (per_group * hdim) + norm_eps)
            for p, x in enumerate(own):
                at = 2 * (g * pairs + p)
                gain = jnp.where(low, gain_buf[at, l:l + 1], gain_buf[at + 1, l:l + 1])
                done.append((x * scale * gain).astype(BF16))
        return jnp.concatenate(done, axis=1)

    stores = []
    for l in range(2):
        value = cur[...]
        x = (value * norm_gain[l:l + 1]).astype(BF16)
        squares = jnp.sum(value * value, axis=1, keepdims=True)
        first = dot(x, local_w[l, 0], NT)
        last = dot(x, local_w[l, 1], NT)
        last = jnp.where(lane == size + 1, squares, last)
        for j in range(dp):
            rs_send[l, j, :, 0:LANES] = first[j * seq:(j + 1) * seq].astype(BF16)
            rs_send[l, j, :, 3 * LANES:] = last[j * seq:(j + 1) * seq].astype(BF16)
        for copy in got_wr[l]:
            copy.wait_recv()
        for kind in range(2):
            mid = dot(x, wr_buf[l, kind].reshape(nstate, feats), NT)
            for j in range(dp):
                rs_send[l, j, :, (1 + kind) * LANES:(2 + kind) * LANES] = mid[j * seq:(j + 1) * seq].astype(BF16)
        got = []
        for i in range(1, dp):
            to = lax.rem(d + i, dp)
            copy = pltpu.make_async_remote_copy(
                src_ref=rs_send.at[l, to], dst_ref=rs_buf.at[l, d], send_sem=rs_ssem.at[l, i - 1],
                recv_sem=rs_rsem.at[l, i - 1], device_id={"tp": t, "dp": to}, device_id_type=MESH)
            copy.start()
            got.append(copy)
        sent.extend(got)
        if l == 0:
            bulk[OUT0] = middle_hops(OUT0, bulk[OUT0])
            bulk[WR1] = hop(WR1, 0)
            bulk[OUT1] = hop(OUT1, 0)
        else:
            got_out[1] = last_hop(OUT1, bulk[OUT1])
        rs_buf[l, d] = rs_send[l, d]
        value_hist = sum(
            hist_value[l, k].astype(F32) * live[k] * tap_value[l, k:k + 1] for k in range(hist_len))
        if l == 0:
            for copy in got_conv + got_gain:
                copy.wait_recv()
            got_out[0] = last_hop(OUT0, bulk[OUT0])
            convs = [conv_buf[kind].reshape(nstate, LANES).astype(F32).T for kind in range(2)]
        for copy in got:
            copy.wait_recv()
        if l == 0:
            bulk[WR1] = middle_hops(WR1, bulk[WR1])
        z = sum(rs_buf[l, j].astype(F32) for j in range(dp))
        z = z * lax.rsqrt(z[:, 3 * LANES + size + 1:3 * LANES + size + 2] / total + norm_eps)
        step_raw = z[:, 3 * LANES + size:3 * LANES + size + 1]
        z16 = z.astype(BF16)
        zr = z16.astype(F32)
        fresh[l, :, 0:LANES] = z16[:, 0:LANES]
        fresh[l, :, LANES:] = z16[:, 3 * LANES:]
        acts = []
        for kind in range(2):
            base = convs[kind][l * span:l * span + seq]
            tap = convs[kind][l * span + seq:l * span + seq + 1]
            acts.append(sigmoid_mul(base + tap * zr[:, (1 + kind) * LANES:(2 + kind) * LANES]))
        write, read = acts
        u = sigmoid_mul(value_hist + tap_value[l, hist_len:hist_len + 1] * zr[:, 0:vcols])
        gate = zr[:, vcols:2 * vcols]
        pre = step_raw + step_bias[:, l:l + 1]
        step = jnp.maximum(pre, 0.0) + jnp.log1p(jnp.exp(-jnp.abs(pre)))
        keep = jnp.exp(-decay_rate[:, l:l + 1] * step)
        read16 = read.astype(BF16)
        held = jnp.zeros((seq, 2 * hdim), F32)
        which = iota((seq, 1), 0)
        for j in range(seq // 2):
            part = dot(read16, stb[l, 2 * j * hdim:2 * (j + 1) * hdim, :], NT)
            held = jnp.where(which // 2 == j, part, held)
        held = jnp.where(which % 2 == 0, held[:, :hdim], held[:, hdim:])
        su = step * u
        overlap = jnp.sum(write * read, axis=1, keepdims=True)
        readout = keep * held + su * overlap + skip_gain[:, l:l + 1] * u
        gated = readout * sigmoid_mul(gate)
        aux[l, :, 0:nstate] = write
        aux[l, :, nstate:] = jnp.concatenate([su, jnp.broadcast_to(keep, (seq, hdim))], axis=1)
        stores.append(pltpu.make_async_copy(aux.at[l], aux_out.at[l], out_sem.at[2 * l]))
        stores.append(pltpu.make_async_copy(fresh.at[l], fresh_out.at[l], out_sem.at[2 * l + 1]))
        mix_send[l] = jnp.concatenate([gated[:packed], gated[seq - packed:]], axis=1).astype(BF16)
        if l == 0:
            got = []
            for j in range(dp):
                for i in range(tp):
                    if i + j == 0:
                        continue
                    copy = pltpu.make_async_remote_copy(
                        src_ref=mix_send.at[0], dst_ref=mix_buf.at[d, t],
                        send_sem=mix_ssem.at[j * tp + i - 1], recv_sem=mix_rsem.at[j * tp + i - 1],
                        device_id={"tp": lax.rem(t + i, tp), "dp": lax.rem(d + j, dp)}, device_id_type=MESH)
                    copy.start()
                    got.append(copy)
            sent.extend(got)
            mix_buf[d, t] = mix_send[0]
            got_wr[1] = last_hop(WR1, bulk[WR1])
            bulk[OUT1] = middle_hops(OUT1, bulk[OUT1])
            for copy in got_out[0]:
                copy.wait_recv()
            for copy in got:
                copy.wait_recv()
            lhs = jnp.concatenate(
                [normed_rows(lambda i, j=j: mix_buf[j, i], 0) for j in range(dp)], axis=0)
            full = dot(lhs, out_buf[0].reshape(tp * vcols, feats))
            cur[...] = full.astype(BF16).astype(F32)

    def last_copy(j, m):
        to = k_blocks * d + m
        return to, pltpu.make_async_remote_copy(
            src_ref=mix_send.at[1], dst_ref=last_buf.at[t], send_sem=last_ssem.at[j * k_blocks + m],
            recv_sem=last_rsem.at[t], device_id={"tp": to, "dp": lax.rem(d + j, dp)}, device_id_type=MESH)

    for j in range(dp):
        for m in range(k_blocks):
            to, copy = last_copy(j, m)
            if j == 0:
                pl.when(to != t)(copy.start)
            else:
                copy.start()
    for copy in stores:
        copy.start()
    for copy in got_out[1]:
        copy.wait_recv()

    def arrived(i):
        pltpu.make_async_remote_copy(
            src_ref=mix_send.at[1], dst_ref=last_buf.at[i], send_sem=last_ssem.at[0],
            recv_sem=last_rsem.at[i], device_id={"tp": t, "dp": lax.rem(d + 1, dp)},
            device_id_type=MESH).wait_recv()

    for i in range(1, tp):
        arrived(lax.rem(t + i, tp))
    is_mine = t // k_blocks == d
    pl.when(jnp.logical_not(is_mine))(lambda: arrived(t))

    @pl.when(is_mine)
    def _():
        last_buf[t] = mix_send[1]

    full = dot(normed_rows(lambda i: last_buf[i], 1), out_buf[1].reshape(tp * vcols, feats))
    mine = full[:rows]
    for m in range(1, k_blocks):
        mine = jnp.where(t % k_blocks == m, full[m * rows:(m + 1) * rows], mine)
    mixed[...] = mine
    stores.append(pltpu.make_async_copy(mixed, mixed_out, out_sem.at[4]))
    stores[-1].start()

    for copy in sent:
        copy.wait_send()
    for j in range(dp):
        for m in range(k_blocks):
            to, copy = last_copy(j, m)
            if j == 0:
                pl.when(to != t)(copy.wait_send)
            else:
                copy.wait_send()
    for copy in stores:
        copy.wait()


def finish_kernel(chunk, *refs):
    ins, outs, held, made = refs[:8], refs[8:13], refs[13:21], refs[21:26]
    in_sem, st_sem, out_sem, new_sem = refs[26:]
    lengths, mixed_in, aux, fresh, state, hist_value, hist_write, hist_read = held
    mixed, new_state, new_value, new_write, new_read = made
    hist_len, seq, vcols = hist_value.shape[1:]
    wcols = hist_write.shape[-1]
    nstate = state.shape[-1]
    hdim = state.shape[-2]
    places = [(l, at) for l in range(2) for at in range(0, seq, chunk)]
    small = [i for i in range(8) if i != 4]
    loads = {i: pltpu.make_async_copy(ins[i], held[i], in_sem.at[i]) for i in small}
    blocks = []
    stores = []
    loads[2].start()
    for n, (l, at) in enumerate(places):
        blocks.append(pltpu.make_async_copy(
            ins[4].at[l, at:at + chunk], state.at[l, at:at + chunk], st_sem.at[n]))
        blocks[-1].start()
    for i in small:
        if i != 2:
            loads[i].start()
    loads[2].wait()
    for n, (l, at) in enumerate(places):
        write = aux[l, at:at + chunk, 0:nstate]
        rest = aux[l, at:at + chunk, nstate:].T
        blocks[n].wait()
        for s in range(chunk):
            su = rest[0:hdim, s:s + 1]
            keep = rest[hdim:, s:s + 1]
            new_state[l, at + s] = keep * state[l, at + s] + su * write[s:s + 1]
        stores.append(pltpu.make_async_copy(
            new_state.at[l, at:at + chunk], outs[1].at[l, at:at + chunk], new_sem.at[n]))
        stores[-1].start()
        if n == 0:
            for i in small:
                if i != 2:
                    loads[i].wait()
            live = live_columns(lengths[...], seq, hist_len)
            mixed[...] = mixed_in[...]
            edges = (
                (hist_value, new_value, 0, vcols),
                (hist_write, new_write, LANES, wcols),
                (hist_read, new_read, LANES + wcols, wcols),
            )
            for old, new, edge, width in edges:
                for m in range(2):
                    for k in range(1, hist_len):
                        new[m, k - 1] = (old[m, k].astype(F32) * live[k]).astype(BF16)
                    new[m, hist_len - 1] = fresh[m, :, edge:edge + width]
            for i in (0, 2, 3, 4):
                stores.append(pltpu.make_async_copy(made[i], outs[i], out_sem.at[i]))
                stores[-1].start()
    for copy in stores:
        copy.wait()


def body(tp, dp, tokens, lengths, norm_gain, w_gate, w_value, w_write, w_read, w_step, step_bias,
         decay_rate, skip_gain, conv_value_w, conv_write_w, conv_read_w, group_gain, w_out, state,
         hist_value, hist_write, hist_read):
    rows, feats = tokens.shape
    seq = state.shape[1]
    hdim, nstate = state.shape[3:]
    hist_len = hist_value.shape[2]
    vcols, wcols = w_value.shape[2], w_write.shape[2]
    cj = wcols // GROUPS
    packed = 16
    chunk = 8
    lens = lengths.reshape(1, seq)
    flip = functools.partial(jnp.swapaxes, axis1=1, axis2=2)
    state4 = state.reshape(2, seq, hdim, nstate)
    hists = [flip(h) for h in (hist_value, hist_write, hist_read)]
    aspec = pl.BlockSpec(memory_space=pl.ANY)
    dma = pltpu.SemaphoreType.DMA
    operands = (
        tokens, lens, norm_gain, flip(w_gate), flip(w_value), flip(w_write), flip(w_read),
        jnp.transpose(w_step, (2, 0, 1)).reshape(2, feats), step_bias.T, decay_rate.T, skip_gain.T,
        conv_value_w, conv_write_w, conv_read_w, group_gain, w_out, state4, *hists)
    results = (
        jax.ShapeDtypeStruct((rows, feats), F32),
        jax.ShapeDtypeStruct((2, seq, nstate + 2 * hdim), F32),
        jax.ShapeDtypeStruct((2, seq, 2 * LANES), BF16),
    )
    mixed, aux, fresh = pl.pallas_call(
        functools.partial(mixer_kernel, tp, dp),
        out_shape=results,
        in_specs=[aspec] * len(operands),
        out_specs=(aspec,) * 3,
        scratch_shapes=[
            *[VMEM(x.shape, x.dtype) for x in operands],
            *[VMEM(x.shape, x.dtype) for x in results],
            dma((len(operands),)),
            dma((5,)),
            VMEM((tp, rows, feats), BF16),
            VMEM((2, GROUPS, 2, cj, feats), BF16),
            VMEM((2, 2, tp, cj, feats), BF16),
            VMEM((GROUPS, 2, cj, LANES), BF16),
            VMEM((2, tp, cj, LANES), BF16),
            VMEM((2, LANES), F32),
            VMEM((tp, 2, LANES), F32),
            VMEM((2, tp, vcols, feats), BF16),
            VMEM((2, 2, LANES, feats), BF16),
            VMEM((seq * dp, feats), F32),
            VMEM((2, dp, seq, 4 * LANES), BF16),
            VMEM((2, dp, seq, 4 * LANES), BF16),
            VMEM((2, packed, LANES), BF16),
            VMEM((dp, tp, packed, LANES), BF16),
            VMEM((tp, packed, LANES), BF16),
            VMEM((2, seq * hdim, nstate), BF16),
            dma((7, tp - 1)),
            dma((7, tp - 1)),
            dma((2, dp - 1)),
            dma((2, dp - 1)),
            dma((tp * dp - 1,)),
            dma((tp * dp - 1,)),
            dma((tp,)),
            dma((tp,)),
        ],
        compiler_params=pltpu.CompilerParams(
            collective_id=0, has_side_effects=True),
        name="mixer_blocks",
    )(*operands)

    given = (lens, mixed, aux, fresh, state4, *hists)
    final = (
        jax.ShapeDtypeStruct(mixed.shape, F32),
        jax.ShapeDtypeStruct(state4.shape, F32),
        *[jax.ShapeDtypeStruct(h.shape, BF16) for h in hists],
    )
    pieces = 2 * (seq // chunk)
    mixed, new_state, *fresh_hists = pl.pallas_call(
        functools.partial(finish_kernel, chunk),
        out_shape=final,
        in_specs=[aspec] * len(given),
        out_specs=(aspec,) * len(final),
        scratch_shapes=[
            *[VMEM(x.shape, x.dtype) for x in given + final],
            dma((len(given),)),
            dma((pieces,)),
            dma((len(final),)),
            dma((pieces,)),
        ],
        name="new_states",
    )(*given)
    return (mixed, new_state.reshape(state.shape), *[flip(h) for h in fresh_hists])


def solution(mesh):
    columns = P(None, "dp", "tp")
    heads = P(None, "tp")
    taps = P(None, None, "tp")
    states = P(None, "dp", "tp", None, None)
    history = P(None, "dp", None, "tp")
    in_specs = (
        P("tp", "dp"), P("dp"), P(None, "dp"), columns, columns, columns, columns, columns,
        heads, heads, heads, taps, taps, taps, heads, P(None, "tp", "dp"), states,
        history, history, history,
    )
    out_specs = (P("tp", "dp"), states, history, history, history)
    run = functools.partial(body, mesh.shape["tp"], mesh.shape["dp"])
    return jax.shard_map(run, mesh=mesh, in_specs=in_specs, out_specs=out_specs, check_vma=False)
```

```python
import functools

import jax
import jax.numpy as jnp
from jax import lax
from jax.experimental import pallas as pl
from jax.experimental.pallas import tpu as pltpu
from jax.sharding import PartitionSpec as P

GROUPS = 2
norm_eps = 1e-05
MESH = pl.DeviceIdType.MESH
VMEM = pltpu.VMEM
LANES = 128
TOK, WR0, CONV, GAIN, OUT0, WR1, OUT1 = range(7)
F32 = jnp.float32
BF16 = jnp.bfloat16

NT = (((1,), (1,)), ((), ()))
NN = (((1,), (0,)), ((), ()))


def dot(a, b, dims=NN, **kw):
    return lax.dot_general(a, b, dims, preferred_element_type=F32, **kw)


def sigmoid_mul(x):
    return x * (1.0 / (1.0 + jnp.exp(-x)))


def iota(shape, axis):
    return lax.broadcasted_iota(jnp.int32, shape, axis)


def live_columns(lengths, seq, hist_len):
    row = jnp.broadcast_to(lengths.astype(F32), (seq, seq))
    same = iota((seq, seq), 0) == iota((seq, seq), 1)
    column = jnp.sum(jnp.where(same, row, 0.0), axis=1, keepdims=True)
    return [(column >= float(hist_len - k)).astype(F32) for k in range(hist_len)]


def mixer_kernel(
    tp, dp, *refs,
):
    count = 20
    held_in = refs[:count]
    mixed_out, aux_out, fresh_out = refs[count:count + 3]
    local = refs[count + 3:2 * count + 3]
    (
        tokens, lengths, norm_gain, w_gate, w_value, w_write, w_read, w_step, step_bias,
        decay_rate, skip_gain, tap_value, tap_write, tap_read, group_gain, w_out, st,
        hist_value, hist_write, hist_read,
    ) = local
    (
    mixed, aux, fresh, in_sem, out_sem,
    tok_buf, wr_send, wr_buf, conv_send, conv_buf, gain_send, gain_buf, out_buf,
    local_w, cur, rs_send, rs_buf, mix_send, mix_buf, last_buf, stb,
    tp_send, tp_recv, rs_ssem, rs_rsem, mix_ssem, mix_rsem, last_ssem, last_rsem,
    ) = refs[2 * count + 3:]
    loads = [pltpu.make_async_copy(a, b, in_sem.at[i]) for i, (a, b) in enumerate(zip(held_in, local))]
    t = lax.axis_index("tp")
    d = lax.axis_index("dp")
    rows = tokens.shape[0]
    hist_len, seq, vcols = hist_value.shape[1:]
    wcols = w_write.shape[1]
    cj = wcols // GROUPS
    nstate = st.shape[-1]
    hdim = st.shape[-2]
    feats = tokens.shape[1]
    total = feats * dp
    seqs = seq * dp
    per_group = tp // GROUPS
    group = t // per_group
    k_blocks = tp // dp
    packed = mix_send.shape[1]
    lane = iota((1, LANES), 1)
    low = lane < hdim

    barrier = pltpu.get_barrier_semaphore()
    for i in range(1, tp):
        pl.semaphore_signal(barrier, inc=1, device_id={"tp": lax.rem(t + i, tp), "dp": d}, device_id_type=MESH)
    for i in range(1, dp):
        pl.semaphore_signal(barrier, inc=1, device_id={"tp": t, "dp": lax.rem(d + i, dp)}, device_id_type=MESH)
    early = (0, 5, 6)
    middle = (1, 11, 12, 13, 14, 17, 18, 19, 15)
    late = tuple(i for i in range(count) if i not in early + middle and i != 16)
    for i in early + middle + late + (16,):
        loads[i].start()
    for i in early:
        loads[i].wait()

    size = 2 * wcols
    r, c = iota((size, size), 0), iota((size, size), 1)
    source = ((r // cj) % 2) * wcols + (r % cj) * GROUPS + r // (2 * cj)
    pick = (c == source).astype(F32)
    pick16 = pick.astype(BF16)
    for l in range(2):
        both = jnp.concatenate([w_write[l], w_read[l]], axis=0)
        got = dot(pick16, both).astype(BF16)
        for g in range(GROUPS):
            for kind in range(2):
                at = (g * 2 + kind) * cj
                wr_send[l, g, kind] = got[at:at + cj]

    pl.semaphore_wait(barrier, tp + dp - 2)
    sent = []

    def spread(cat, src_of, dst):
        out = []
        for i in range(1, tp):
            to = lax.rem(t + i, tp)
            copy = pltpu.make_async_remote_copy(
                src_ref=src_of(to), dst_ref=dst, send_sem=tp_send.at[cat, i - 1],
                recv_sem=tp_recv.at[cat, i - 1], device_id={"tp": to, "dp": d}, device_id_type=MESH)
            copy.start()
            out.append(copy)
        sent.extend(out)
        return out

    got_tok = spread(TOK, lambda to: tokens, tok_buf.at[t])
    got_wr = [spread(WR0, lambda to: wr_send.at[0, to // per_group], wr_buf.at[0, :, t]), []]
    got_out = [[], []]

    def flipped(index, bit):
        return index + bit * (1 - 2 * ((index // bit) % 2))

    def hop(cat, n):
        bit = tp >> (n + 1)
        to = flipped(t, bit)
        held = [t]
        for m in range(n):
            held = held + [flipped(h, tp >> (m + 1)) for h in held]
        out = []
        for i, h in enumerate(held):
            if cat == WR1:
                src = wr_send.at[1, 1 - group] if n == 0 else wr_buf.at[1, :, h]
                dst = wr_buf.at[1, :, h]
            else:
                layer = 0 if cat == OUT0 else 1
                dst = out_buf.at[layer, h]
                src = w_out.at[layer] if n == 0 else dst
            copy = pltpu.make_async_remote_copy(
                src_ref=src, dst_ref=dst, send_sem=tp_send.at[cat, (1 << n) - 1 + i],
                recv_sem=tp_recv.at[cat, (1 << n) - 1 + i], device_id={"tp": to, "dp": d}, device_id_type=MESH)
            copy.start()
            out.append(copy)
        sent.extend(out)
        return out

    rounds = tp.bit_length() - 1

    def middle_hops(cat, got):
        for n in range(1, rounds - 1):
            for copy in got:
                copy.wait_recv()
            got = hop(cat, n)
        return got

    def last_hop(cat, got):
        for copy in got:
            copy.wait_recv()
        return hop(cat, rounds - 1)


    for i in middle:
        loads[i].wait()
    live = live_columns(lengths[...], seq, hist_len)
    pieces = []
    for l in range(2):
        parts = []
        for hist, tap in ((hist_write, tap_write), (hist_read, tap_read)):
            total_c = sum(hist[l, k].astype(F32) * live[k] * tap[l, k:k + 1] for k in range(hist_len))
            last = tap[l, hist_len:hist_len + 1]
            parts.append(jnp.concatenate([total_c, last, jnp.zeros((7, wcols), F32)], axis=0))
        pieces.append(jnp.concatenate(parts, axis=1))
    span = seq + 8
    pieces.append(jnp.zeros((LANES - 2 * span, size), F32))
    moved = dot(pick, jnp.concatenate(pieces, axis=0), NT, precision=lax.Precision.HIGHEST)
    for g in range(GROUPS):
        for kind in range(2):
            at = (g * 2 + kind) * cj
            conv_send[g, kind] = moved[at:at + cj].astype(BF16)
    gg = group_gain[...]
    gain_send[...] = jnp.concatenate([gg, gg], axis=1)
    got_conv = spread(CONV, lambda to: conv_send.at[to // per_group], conv_buf.at[:, t])
    got_gain = spread(GAIN, lambda to: gain_send, gain_buf.at[t])

    bulk = {OUT0: hop(OUT0, 0)}
    for i in late:
        loads[i].wait()
    tok_buf[t] = tokens[...]
    conv_buf[:, t] = conv_send[group]
    gain_buf[t] = gain_send[...]
    for l in range(2):
        wr_buf[l, :, t] = wr_send[l, group]
        out_buf[l, t] = w_out[l]
        local_w[l, 0] = jnp.concatenate([w_value[l], w_gate[l]], axis=0)
        local_w[l, 1] = jnp.concatenate(
            [w_write[l], w_read[l], w_step[l:l + 1], jnp.zeros((LANES - size - 1, feats), BF16)], axis=0)
    loads[16].wait()
    for l in range(2):
        stb[l] = st[l].reshape(seq * hdim, nstate).astype(BF16)

    for copy in got_tok:
        copy.wait_recv()
    for i in range(tp):
        cur[i * rows:(i + 1) * rows] = tok_buf[i].astype(F32)

    def pair_rows(get, p):
        a, b = get(2 * p).astype(F32), get(2 * p + 1).astype(F32)
        ra, rb = pltpu.roll(a, hdim, 1), pltpu.roll(b, hdim, 1)
        cut = 2 * packed - seq
        return jnp.concatenate([jnp.where(low, a, rb), jnp.where(low, ra, b)[cut:]], axis=0)

    def normed_rows(get, l):
        cols = [pair_rows(get, p) for p in range(tp // 2)]
        pairs = tp // 2 // GROUPS
        done = []
        for g in range(GROUPS):
            own = cols[g * pairs:(g + 1) * pairs]
            sq = sum(jnp.sum(x * x, axis=1, keepdims=True) for x in own)
            scale = lax.rsqrt(sq / (per_group * hdim) + norm_eps)
            for p, x in enumerate(own):
                at = 2 * (g * pairs + p)
                gain = jnp.where(low, gain_buf[at, l:l + 1], gain_buf[at + 1, l:l + 1])
                done.append((x * scale * gain).astype(BF16))
        return jnp.concatenate(done, axis=1)

    stores = []
    for l in range(2):
        value = cur[...]
        x = (value * norm_gain[l:l + 1]).astype(BF16)
        squares = jnp.sum(value * value, axis=1, keepdims=True)
        first = dot(x, local_w[l, 0], NT)
        last = dot(x, local_w[l, 1], NT)
        last = jnp.where(lane == size + 1, squares, last)
        for j in range(dp):
            rs_send[l, j, :, 0:LANES] = first[j * seq:(j + 1) * seq].astype(BF16)
            rs_send[l, j, :, 3 * LANES:] = last[j * seq:(j + 1) * seq].astype(BF16)
        for copy in got_wr[l]:
            copy.wait_recv()
        for kind in range(2):
            mid = dot(x, wr_buf[l, kind].reshape(nstate, feats), NT)
            for j in range(dp):
                rs_send[l, j, :, (1 + kind) * LANES:(2 + kind) * LANES] = mid[j * seq:(j + 1) * seq].astype(BF16)
        got = []
        for i in range(1, dp):
            to = lax.rem(d + i, dp)
            copy = pltpu.make_async_remote_copy(
                src_ref=rs_send.at[l, to], dst_ref=rs_buf.at[l, d], send_sem=rs_ssem.at[l, i - 1],
                recv_sem=rs_rsem.at[l, i - 1], device_id={"tp": t, "dp": to}, device_id_type=MESH)
            copy.start()
            got.append(copy)
        sent.extend(got)
        if l == 0:
            bulk[WR1] = hop(WR1, 0)
            bulk[OUT1] = hop(OUT1, 0)
        else:
            got_out[1] = last_hop(OUT1, bulk[OUT1])
        rs_buf[l, d] = rs_send[l, d]
        value_hist = sum(
            hist_value[l, k].astype(F32) * live[k] * tap_value[l, k:k + 1] for k in range(hist_len))
        if l == 0:
            for copy in got_conv + got_gain:
                copy.wait_recv()
            convs = [conv_buf[kind].reshape(nstate, LANES).astype(F32).T for kind in range(2)]
        for copy in got:
            copy.wait_recv()
        if l == 0:
            bulk[OUT0] = middle_hops(OUT0, bulk[OUT0])
        z = sum(rs_buf[l, j].astype(F32) for j in range(dp))
        z = z * lax.rsqrt(z[:, 3 * LANES + size + 1:3 * LANES + size + 2] / total + norm_eps)
        step_raw = z[:, 3 * LANES + size:3 * LANES + size + 1]
        z16 = z.astype(BF16)
        zr = z16.astype(F32)
        fresh[l, :, 0:LANES] = z16[:, 0:LANES]
        fresh[l, :, LANES:] = z16[:, 3 * LANES:]
        acts = []
        for kind in range(2):
            base = convs[kind][l * span:l * span + seq]
            tap = convs[kind][l * span + seq:l * span + seq + 1]
            acts.append(sigmoid_mul(base + tap * zr[:, (1 + kind) * LANES:(2 + kind) * LANES]))
        write, read = acts
        u = sigmoid_mul(value_hist + tap_value[l, hist_len:hist_len + 1] * zr[:, 0:vcols])
        gate = zr[:, vcols:2 * vcols]
        pre = step_raw + step_bias[:, l:l + 1]
        step = jnp.maximum(pre, 0.0) + jnp.log1p(jnp.exp(-jnp.abs(pre)))
        keep = jnp.exp(-decay_rate[:, l:l + 1] * step)
        read16 = read.astype(BF16)
        held = jnp.zeros((seq, 2 * hdim), F32)
        which = iota((seq, 1), 0)
        for j in range(seq // 2):
            part = dot(read16, stb[l, 2 * j * hdim:2 * (j + 1) * hdim, :], NT)
            held = jnp.where(which // 2 == j, part, held)
        held = jnp.where(which % 2 == 0, held[:, :hdim], held[:, hdim:])
        su = step * u
        overlap = jnp.sum(write * read, axis=1, keepdims=True)
        readout = keep * held + su * overlap + skip_gain[:, l:l + 1] * u
        gated = readout * sigmoid_mul(gate)
        aux[l, :, 0:nstate] = write
        aux[l, :, nstate:] = jnp.concatenate([su, jnp.broadcast_to(keep, (seq, hdim))], axis=1)
        stores.append(pltpu.make_async_copy(aux.at[l], aux_out.at[l], out_sem.at[2 * l]))
        stores.append(pltpu.make_async_copy(fresh.at[l], fresh_out.at[l], out_sem.at[2 * l + 1]))
        mix_send[l] = jnp.concatenate([gated[:packed], gated[seq - packed:]], axis=1).astype(BF16)
        if l == 0:
            got = []
            for j in range(dp):
                for i in range(tp):
                    if i + j == 0:
                        continue
                    copy = pltpu.make_async_remote_copy(
                        src_ref=mix_send.at[0], dst_ref=mix_buf.at[d, t],
                        send_sem=mix_ssem.at[j * tp + i - 1], recv_sem=mix_rsem.at[j * tp + i - 1],
                        device_id={"tp": lax.rem(t + i, tp), "dp": lax.rem(d + j, dp)}, device_id_type=MESH)
                    copy.start()
                    got.append(copy)
            sent.extend(got)
            mix_buf[d, t] = mix_send[0]
            bulk[WR1] = middle_hops(WR1, bulk[WR1])
            got_out[0] = last_hop(OUT0, bulk[OUT0])
            bulk[OUT1] = middle_hops(OUT1, bulk[OUT1])
            got_wr[1] = last_hop(WR1, bulk[WR1])
            for copy in got_out[0]:
                copy.wait_recv()
            for copy in got:
                copy.wait_recv()
            lhs = jnp.concatenate(
                [normed_rows(lambda i, j=j: mix_buf[j, i], 0) for j in range(dp)], axis=0)
            full = dot(lhs, out_buf[0].reshape(tp * vcols, feats))
            cur[...] = full.astype(BF16).astype(F32)

    def last_copy(j, m):
        to = k_blocks * d + m
        return to, pltpu.make_async_remote_copy(
            src_ref=mix_send.at[1], dst_ref=last_buf.at[t], send_sem=last_ssem.at[j * k_blocks + m],
            recv_sem=last_rsem.at[t], device_id={"tp": to, "dp": lax.rem(d + j, dp)}, device_id_type=MESH)

    for j in range(dp):
        for m in range(k_blocks):
            to, copy = last_copy(j, m)
            if j == 0:
                pl.when(to != t)(copy.start)
            else:
                copy.start()
    for copy in stores:
        copy.start()
    for copy in got_out[1]:
        copy.wait_recv()

    def arrived(i):
        pltpu.make_async_remote_copy(
            src_ref=mix_send.at[1], dst_ref=last_buf.at[i], send_sem=last_ssem.at[0],
            recv_sem=last_rsem.at[i], device_id={"tp": t, "dp": lax.rem(d + 1, dp)},
            device_id_type=MESH).wait_recv()

    for i in range(1, tp):
        arrived(lax.rem(t + i, tp))
    is_mine = t // k_blocks == d
    pl.when(jnp.logical_not(is_mine))(lambda: arrived(t))

    @pl.when(is_mine)
    def _():
        last_buf[t] = mix_send[1]

    full = dot(normed_rows(lambda i: last_buf[i], 1), out_buf[1].reshape(tp * vcols, feats))
    mine = full[:rows]
    for m in range(1, k_blocks):
        mine = jnp.where(t % k_blocks == m, full[m * rows:(m + 1) * rows], mine)
    mixed[...] = mine
    stores.append(pltpu.make_async_copy(mixed, mixed_out, out_sem.at[4]))
    stores[-1].start()

    for copy in sent:
        copy.wait_send()
    for j in range(dp):
        for m in range(k_blocks):
            to, copy = last_copy(j, m)
            if j == 0:
                pl.when(to != t)(copy.wait_send)
            else:
                copy.wait_send()
    for copy in stores:
        copy.wait()


def finish_kernel(chunk, *refs):
    ins, outs, held, made = refs[:8], refs[8:13], refs[13:21], refs[21:26]
    in_sem, st_sem, out_sem, new_sem = refs[26:]
    lengths, mixed_in, aux, fresh, state, hist_value, hist_write, hist_read = held
    mixed, new_state, new_value, new_write, new_read = made
    hist_len, seq, vcols = hist_value.shape[1:]
    wcols = hist_write.shape[-1]
    nstate = state.shape[-1]
    hdim = state.shape[-2]
    places = [(l, at) for l in range(2) for at in range(0, seq, chunk)]
    small = [i for i in range(8) if i != 4]
    loads = {i: pltpu.make_async_copy(ins[i], held[i], in_sem.at[i]) for i in small}
    blocks = []
    stores = []
    loads[2].start()
    for n, (l, at) in enumerate(places):
        blocks.append(pltpu.make_async_copy(
            ins[4].at[l, at:at + chunk], state.at[l, at:at + chunk], st_sem.at[n]))
        blocks[-1].start()
    for i in small:
        if i != 2:
            loads[i].start()
    loads[2].wait()
    for n, (l, at) in enumerate(places):
        write = aux[l, at:at + chunk, 0:nstate]
        rest = aux[l, at:at + chunk, nstate:].T
        blocks[n].wait()
        for s in range(chunk):
            su = rest[0:hdim, s:s + 1]
            keep = rest[hdim:, s:s + 1]
            new_state[l, at + s] = keep * state[l, at + s] + su * write[s:s + 1]
        stores.append(pltpu.make_async_copy(
            new_state.at[l, at:at + chunk], outs[1].at[l, at:at + chunk], new_sem.at[n]))
        stores[-1].start()
        if n == 0:
            for i in small:
                if i != 2:
                    loads[i].wait()
            live = live_columns(lengths[...], seq, hist_len)
            mixed[...] = mixed_in[...]
            edges = (
                (hist_value, new_value, 0, vcols),
                (hist_write, new_write, LANES, wcols),
                (hist_read, new_read, LANES + wcols, wcols),
            )
            for old, new, edge, width in edges:
                for m in range(2):
                    for k in range(1, hist_len):
                        new[m, k - 1] = (old[m, k].astype(F32) * live[k]).astype(BF16)
                    new[m, hist_len - 1] = fresh[m, :, edge:edge + width]
            for i in (0, 2, 3, 4):
                stores.append(pltpu.make_async_copy(made[i], outs[i], out_sem.at[i]))
                stores[-1].start()
    for copy in stores:
        copy.wait()


def body(tp, dp, tokens, lengths, norm_gain, w_gate, w_value, w_write, w_read, w_step, step_bias,
         decay_rate, skip_gain, conv_value_w, conv_write_w, conv_read_w, group_gain, w_out, state,
         hist_value, hist_write, hist_read):
    rows, feats = tokens.shape
    seq = state.shape[1]
    hdim, nstate = state.shape[3:]
    hist_len = hist_value.shape[2]
    vcols, wcols = w_value.shape[2], w_write.shape[2]
    cj = wcols // GROUPS
    packed = 16
    chunk = 8
    lens = lengths.reshape(1, seq)
    flip = functools.partial(jnp.swapaxes, axis1=1, axis2=2)
    state4 = state.reshape(2, seq, hdim, nstate)
    hists = [flip(h) for h in (hist_value, hist_write, hist_read)]
    aspec = pl.BlockSpec(memory_space=pl.ANY)
    dma = pltpu.SemaphoreType.DMA
    operands = (
        tokens, lens, norm_gain, flip(w_gate), flip(w_value), flip(w_write), flip(w_read),
        jnp.transpose(w_step, (2, 0, 1)).reshape(2, feats), step_bias.T, decay_rate.T, skip_gain.T,
        conv_value_w, conv_write_w, conv_read_w, group_gain, w_out, state4, *hists)
    results = (
        jax.ShapeDtypeStruct((rows, feats), F32),
        jax.ShapeDtypeStruct((2, seq, nstate + 2 * hdim), F32),
        jax.ShapeDtypeStruct((2, seq, 2 * LANES), BF16),
    )
    mixed, aux, fresh = pl.pallas_call(
        functools.partial(mixer_kernel, tp, dp),
        out_shape=results,
        in_specs=[aspec] * len(operands),
        out_specs=(aspec,) * 3,
        scratch_shapes=[
            *[VMEM(x.shape, x.dtype) for x in operands],
            *[VMEM(x.shape, x.dtype) for x in results],
            dma((len(operands),)),
            dma((5,)),
            VMEM((tp, rows, feats), BF16),
            VMEM((2, GROUPS, 2, cj, feats), BF16),
            VMEM((2, 2, tp, cj, feats), BF16),
            VMEM((GROUPS, 2, cj, LANES), BF16),
            VMEM((2, tp, cj, LANES), BF16),
            VMEM((2, LANES), F32),
            VMEM((tp, 2, LANES), F32),
            VMEM((2, tp, vcols, feats), BF16),
            VMEM((2, 2, LANES, feats), BF16),
            VMEM((seq * dp, feats), F32),
            VMEM((2, dp, seq, 4 * LANES), BF16),
            VMEM((2, dp, seq, 4 * LANES), BF16),
            VMEM((2, packed, LANES), BF16),
            VMEM((dp, tp, packed, LANES), BF16),
            VMEM((tp, packed, LANES), BF16),
            VMEM((2, seq * hdim, nstate), BF16),
            dma((7, tp - 1)),
            dma((7, tp - 1)),
            dma((2, dp - 1)),
            dma((2, dp - 1)),
            dma((tp * dp - 1,)),
            dma((tp * dp - 1,)),
            dma((tp,)),
            dma((tp,)),
        ],
        compiler_params=pltpu.CompilerParams(
            collective_id=0, has_side_effects=True),
        name="mixer_blocks",
    )(*operands)

    given = (lens, mixed, aux, fresh, state4, *hists)
    final = (
        jax.ShapeDtypeStruct(mixed.shape, F32),
        jax.ShapeDtypeStruct(state4.shape, F32),
        *[jax.ShapeDtypeStruct(h.shape, BF16) for h in hists],
    )
    pieces = 2 * (seq // chunk)
    mixed, new_state, *fresh_hists = pl.pallas_call(
        functools.partial(finish_kernel, chunk),
        out_shape=final,
        in_specs=[aspec] * len(given),
        out_specs=(aspec,) * len(final),
        scratch_shapes=[
            *[VMEM(x.shape, x.dtype) for x in given + final],
            dma((len(given),)),
            dma((pieces,)),
            dma((len(final),)),
            dma((pieces,)),
        ],
        name="new_states",
    )(*given)
    return (mixed, new_state.reshape(state.shape), *[flip(h) for h in fresh_hists])


def solution(mesh):
    columns = P(None, "dp", "tp")
    heads = P(None, "tp")
    taps = P(None, None, "tp")
    states = P(None, "dp", "tp", None, None)
    history = P(None, "dp", None, "tp")
    in_specs = (
        P("tp", "dp"), P("dp"), P(None, "dp"), columns, columns, columns, columns, columns,
        heads, heads, heads, taps, taps, taps, heads, P(None, "tp", "dp"), states,
        history, history, history,
    )
    out_specs = (P("tp", "dp"), states, history, history, history)
    run = functools.partial(body, mesh.shape["tp"], mesh.shape["dp"])
    return jax.shard_map(run, mesh=mesh, in_specs=in_specs, out_specs=out_specs, check_vma=False)
```
